32 devices in a mesh: ep: 16 (over z, y, x), tp: 2 (over core).
Axes of the slice: x: 2, y: 2, z: 4, core: 2. Of those that a mesh axis runs over, the one named last changes fastest.
Arguments:
- tokens: bfloat16 [256, 1536], P('ep'), may hold values from -6 to 6
- prior_state: float32 [256, 12, 64, 64], P('ep', 'tp'), may hold values from -12 to 12
- first_gain: float32 [1536], replicated, may hold values from 0.1 to 1.9
- query_weight: bfloat16 [1536, 768], P(None, 'tp'), may hold values from -0.15625 to 0.15625
- key_weight: bfloat16 [1536, 768], P(None, 'tp'), may hold values from -0.15625 to 0.15625
- value_weight: bfloat16 [1536, 768], P(None, 'tp'), may hold values from -0.15625 to 0.15625
- decay_down: bfloat16 [1536, 96], replicated, may hold values from -0.15625 to 0.15625
- decay_up: bfloat16 [96, 768], P(None, 'tp'), may hold values from -1.25 to 1.25
- decay_base: float32 [768], P('tp'), may hold values from -5 to 1
- rate_down: bfloat16 [1536, 96], replicated, may hold values from -0.15625 to 0.15625
- rate_up: bfloat16 [96, 768], P(None, 'tp'), may hold values from -1.25 to 1.25
- rate_base: float32 [768], P('tp'), may hold values from -4 to 4
- head_gain: float32 [768], P('tp'), may hold values from 0.1 to 1.9
- out_weight: bfloat16 [768, 1536], P('tp'), may hold values from -0.21875 to 0.21875
- mid_gain: float32 [1536], replicated, may hold values from 0.1 to 1.9
- route_ids: int32 [256, 6], P('ep'), may hold values from 0 to 15, all different within a row; in each aligned block of 16 rows (0 to 15, 16 to 31, ...) at most 12 rows name the same one
- route_weights: float32 [256, 6], P('ep'), may hold values from 0.1 to 1
- expert_gate: bfloat16 [16, 1536, 384], P('ep', None, 'tp'), may hold values from -0.15625 to 0.15625
- expert_up: bfloat16 [16, 1536, 384], P('ep', None, 'tp'), may hold values from -0.15625 to 0.15625
- expert_down: bfloat16 [16, 384, 1536], P('ep', 'tp'), may hold values from -0.3125 to 0.3125
- dense_gate: bfloat16 [1536, 6144], P(None, ('ep', 'tp')), may hold values from -0.15625 to 0.15625
- dense_up: bfloat16 [1536, 6144], P(None, ('ep', 'tp')), may hold values from -0.15625 to 0.15625
- dense_down: bfloat16 [6144, 1536], P(('ep', 'tp')), may hold values from -0.078125 to 0.078125
- blend_vector: bfloat16 [1536], replicated, may hold values from -0.15625 to 0.15625
Outputs:
- mixed: bfloat16 [256, 1536], P('ep', 'tp')
- new_state: float32 [256, 12, 64, 64], P('ep', 'tp')
The draws below stay inside these ranges and needn't reach their ends.
Inputs may be any that keep to these rules, and one draw needn't show every extreme that they name: `route_ids`: each row names 6 different experts; among the rows of one device no expert is named by more than 12 rows, a bound that some block reaches.
All inputs are finite; a program needn't handle non-finite values.
Results may differ from the reference program's by a relative error of at most 0.02.
Values may be sent and summed in bfloat16 or wider, within the bound.
No kernel may reach another device: no remote copies, remote signals or barrier semaphores. Data moves between devices by JAX's collectives and lax.ppermute only.
A program may use at most 128 MiB of HBM per device.

```python
import math
import jax
import jax.numpy as jnp
import numpy as np
from jax import lax

D = 1536
HEADS = 12
HEAD = 64
INNER = 768
RANK = 96
FE = 384
FD = 6144
TOP = 6
SEQS = 16
EXPERTS = 16
BATCH = 256
CAP = 12
N_EP = 16
N_TP = 2


def levels(key, extent, pieces, least, largest):
    level = 1.0
    for axis_at, parts in pieces:
        draws = jax.random.uniform(jax.random.fold_in(jax.random.fold_in(key, 6), axis_at), (parts,), jnp.float32, least / len(pieces), largest / len(pieces))
        level = level * jnp.repeat(jnp.exp(draws), extent[axis_at] // parts).reshape((-1,) + (1,) * (len(extent) - 1 - axis_at))
    return level


def shared_out(rng, own, number, rows, count, top, bound, slope):
    sequence = jax.random.permutation(rng, count)
    crowded, common = shares(count, rows * top, bound, slope, True), shares(count, rows * top, bound, slope, False)
    places = jnp.arange(count)

    def named(tallies, offset_by):
        used = int((tallies > 0).sum())
        fixed = max(1, used // 4)
        passed = fixed + (places - fixed + offset_by * (used - fixed)) % max(1, count - fixed)
        return jnp.zeros((count,), jnp.int32).at[sequence[jnp.where(places < fixed, places, passed)]].set(jnp.asarray(tallies, jnp.int32))

    tallies = jnp.where(number % 4 == 0, named(crowded, number // 4), named(common, number - number // 4 - 1))
    mixed = jax.random.permutation(jax.random.fold_in(own, 3), count)
    donor, taker = mixed[0:count // 2 * 2:2], mixed[1:count // 2 * 2:2]
    room = jnp.minimum(tallies[donor] - 1, bound - tallies[taker]) // 2
    room = jnp.where((donor == sequence[0]) | (taker == sequence[0]) | (tallies[taker] == 0), 0, jnp.maximum(room, 0))
    passed = jax.random.randint(jax.random.fold_in(own, 4), (count // 2,), 0, 1 << 20) % (room + 1)
    tallies = tallies.at[donor].add(-passed).at[taker].add(passed)
    items = jnp.searchsorted(jnp.cumsum(tallies), jnp.arange(rows * top), side="right").astype(jnp.int32)
    table = items.reshape(top, rows).T
    table = table[jax.random.permutation(jax.random.fold_in(own, 1), rows)]
    offset_by = jax.random.randint(jax.random.fold_in(own, 2), (rows, 1), 0, top)
    return jnp.take_along_axis(table, (jnp.arange(top)[None, :] + offset_by) % top, axis=1)


def shares(amount, total, limit, skew, full):
    portions = [(1 << 20) // math.isqrt(standing ** skew) + 1 for standing in range(1, amount + 1)]
    largest = limit if full else min(limit, max(-(-total // amount), total * portions[0] // sum(portions)))
    least = 1 if total - largest >= amount - 1 else 0
    holding, spare = [largest] + [least] * (amount - 1), total - largest - least * (amount - 1)
    while spare > 0:
        free = [i for i in range(1, amount) if holding[i] < largest] or [i for i in range(1, amount) if holding[i] < limit]
        whole, left = sum([portions[i] for i in free]), spare
        for i in free:
            extra = min(limit - holding[i], max(1, left * portions[i] // whole), spare)
            holding[i] = holding[i] + extra
            spare = spare - extra
    return np.array(holding)


def gaussian(stream_key, shape, width, limit, split=(), kind=jnp.bfloat16):
    result = jax.random.normal(stream_key, shape, jnp.float32) * width
    if len(split) > 0:
        result = levels(stream_key, shape, split, -0.22, 0.18) * result
    return jnp.clip(result, min=-limit, max=limit).astype(kind)


def setup_inputs(seed: int = 0) -> dict:
    key_list = jax.random.split(jax.random.key(seed), 25)
    tokens = gaussian(key_list[0], (BATCH, D), 1.0, 6.0, ((0, 16),))
    prior_state = gaussian(key_list[1], (BATCH, HEADS, HEAD, HEAD), 2.0, 12.0, ((0, 16), (1, 2)), jnp.float32)
    first_gain = jnp.clip(1.0 + 0.18 * jax.random.normal(key_list[2], (D,), jnp.float32), 0.1, 1.9)
    query_weight = gaussian(key_list[3], (D, INNER), D ** -0.5, 0.15625, ((1, 2),))
    key_weight = gaussian(key_list[4], (D, INNER), D ** -0.5, 0.15625, ((1, 2),))
    value_weight = gaussian(key_list[5], (D, INNER), D ** -0.5, 0.15625, ((1, 2),))
    decay_down = gaussian(key_list[6], (D, RANK), D ** -0.5, 0.15625)
    decay_up = gaussian(key_list[7], (RANK, INNER), (RANK // 4) ** -0.5, 1.25, ((1, 2),))
    decay_base = jnp.clip(-5.0 + 6.0 * jax.random.uniform(key_list[8], (INNER,), jnp.float32) ** levels(key_list[8], (INNER,), ((0, 2),), -0.2, 0.2), -5.0, 1.0)
    rate_down = gaussian(key_list[9], (D, RANK), D ** -0.5, 0.15625)
    rate_up = gaussian(key_list[10], (RANK, INNER), (RANK // 4) ** -0.5, 1.25, ((1, 2),))
    rate_base = jnp.clip(jax.random.uniform(key_list[11], (INNER,), jnp.float32, -4.0, 4.0) * levels(key_list[11], (INNER,), ((0, 2),), -0.4, 0.0), -4.0, 4.0)
    head_gain = jnp.clip(1.0 + 0.18 * jax.random.normal(key_list[12], (INNER,), jnp.float32), 0.1, 1.9)
    out_weight = gaussian(key_list[13], (INNER, D), INNER ** -0.5, 0.21875, ((0, 2),))
    mid_gain = jnp.clip(1.0 + 0.18 * jax.random.normal(key_list[14], (D,), jnp.float32), 0.1, 1.9)
    route_ids_keys = jax.random.split(jax.random.fold_in(key_list[15], 1), BATCH // SEQS)
    route_ids_turns = jax.random.permutation(jax.random.fold_in(key_list[15], 3), BATCH // SEQS)
    route_ids = jax.vmap(lambda own, number: shared_out(jax.random.fold_in(key_list[15], 2), own, number, SEQS, EXPERTS, TOP, CAP, 2))(route_ids_keys, route_ids_turns).reshape((BATCH, TOP))
    route_weights = jnp.clip(jnp.exp(math.log(1.0) - 2.3025851 * jax.random.uniform(key_list[16], (BATCH, TOP), jnp.float32) ** levels(key_list[16], (BATCH, TOP), ((0, 16),), -0.2, 0.2)), 0.1, 1.0)
    expert_gate = gaussian(key_list[17], (EXPERTS, D, FE), D ** -0.5, 0.15625, ((0, 16), (2, 2)))
    expert_up = gaussian(key_list[18], (EXPERTS, D, FE), D ** -0.5, 0.15625, ((0, 16), (2, 2)))
    expert_down = gaussian(key_list[19], (EXPERTS, FE, D), FE ** -0.5, 0.3125, ((0, 16), (1, 2)))
    dense_gate = gaussian(key_list[20], (D, FD), D ** -0.5, 0.15625, ((1, 32),))
    dense_up = gaussian(key_list[21], (D, FD), D ** -0.5, 0.15625, ((1, 32),))
    dense_down = gaussian(key_list[22], (FD, D), FD ** -0.5, 0.078125, ((0, 32),))
    blend_vector = gaussian(key_list[23], (D,), D ** -0.5, 0.15625)
    return dict(tokens=tokens, prior_state=prior_state, first_gain=first_gain, query_weight=query_weight, key_weight=key_weight, value_weight=value_weight, decay_down=decay_down, decay_up=decay_up, decay_base=decay_base, rate_down=rate_down, rate_up=rate_up, rate_base=rate_base, head_gain=head_gain, out_weight=out_weight, mid_gain=mid_gain, route_ids=route_ids, route_weights=route_weights, expert_gate=expert_gate, expert_up=expert_up, expert_down=expert_down, dense_gate=dense_gate, dense_up=dense_up, dense_down=dense_down, blend_vector=blend_vector)


def rms_norm(values, gain):
    scale = lax.rsqrt(lax.optimization_barrier(jnp.mean(values * values, axis=-1, keepdims=True)) + 1e-06)
    return values * scale * gain.astype(jnp.float32)

def rounded(values):
    return lax.optimization_barrier(values.astype(jnp.bfloat16)).astype(jnp.float32)

def mixer_core(normed, prior_state, query_weight, key_weight, value_weight, decay_down, decay_up, decay_base, rate_down, rate_up, rate_base, head_gain):
    rows = normed.shape[0]
    heads_here = prior_state.shape[1]
    head_size = prior_state.shape[2]

    def project(weight):
        product = jnp.dot(normed, weight, preferred_element_type=jnp.float32)
        return rounded(product).reshape(rows, heads_here, head_size)
    receptance = project(query_weight)
    key_vec = project(key_weight)
    value_vec = project(value_weight)
    decay_low = jnp.tanh(jnp.dot(normed, decay_down, preferred_element_type=jnp.float32)).astype(jnp.bfloat16)
    decay_log = decay_base + jnp.dot(decay_low, decay_up, preferred_element_type=jnp.float32)
    decay_log = -jax.nn.softplus(-decay_log) - 0.5
    decay_rate = jnp.exp(-jnp.exp(decay_log)).reshape(rows, heads_here, head_size)
    rate_low = jnp.dot(normed, rate_down, preferred_element_type=jnp.float32).astype(jnp.bfloat16)
    learn_rate = jax.nn.sigmoid(rate_base + jnp.dot(rate_low, rate_up, preferred_element_type=jnp.float32))
    learn_rate = learn_rate.reshape(rows, heads_here, head_size)
    unit_key = key_vec * lax.rsqrt(lax.optimization_barrier(jnp.sum(key_vec * key_vec, axis=-1, keepdims=True)) + 1e-06)
    removed = lax.optimization_barrier(jnp.sum(prior_state * unit_key[:, :, None, :], axis=-1))
    new_state = prior_state * decay_rate[:, :, None, :] - removed[..., None] * (unit_key * learn_rate)[:, :, None, :] + value_vec[..., None] * key_vec[:, :, None, :]
    read = lax.optimization_barrier(jnp.sum(new_state * receptance[:, :, None, :], axis=-1))
    center = lax.optimization_barrier(jnp.mean(read, axis=-1, keepdims=True))
    spread = lax.optimization_barrier(jnp.mean(jnp.square(read - center), axis=-1, keepdims=True))
    normal = (read - center) * lax.rsqrt(spread + 0.00064)
    mixed_heads = (normal.reshape(rows, -1) * head_gain.astype(jnp.float32)).astype(jnp.bfloat16)
    return (mixed_heads, new_state)

def reference(tokens, prior_state, first_gain, query_weight, key_weight, value_weight, decay_down, decay_up, decay_base, rate_down, rate_up, rate_base, head_gain, out_weight, mid_gain, route_ids, route_weights, expert_gate, expert_up, expert_down, dense_gate, dense_up, dense_down, blend_vector):
    token_f = tokens.astype(jnp.float32)
    normed = rms_norm(token_f, first_gain).astype(jnp.bfloat16)
    mixed_heads, new_state = mixer_core(normed, prior_state, query_weight, key_weight, value_weight, decay_down, decay_up, decay_base, rate_down, rate_up, rate_base, head_gain)
    block = INNER // N_TP
    attn = jnp.zeros((BATCH, D), jnp.float32)
    for part_idx in range(N_TP):
        lower = part_idx * block
        attn = attn + rounded(jnp.dot(mixed_heads[:, lower:lower + block], out_weight[lower:lower + block], preferred_element_type=jnp.float32))
    resid = rounded(token_f + attn)
    mid = rms_norm(resid, mid_gain).astype(jnp.bfloat16)
    blend = jax.nn.sigmoid(jnp.dot(mid, blend_vector, preferred_element_type=jnp.float32))
    flat_ids = route_ids.reshape(N_EP, SEQS * TOP)
    onehot = (flat_ids[..., None] == jnp.arange(EXPERTS, dtype=jnp.int32)[None, None, :]).astype(jnp.int32)
    before = jnp.cumsum(onehot, axis=1) - onehot
    position = lax.optimization_barrier(jnp.sum(onehot * before, axis=-1))
    group_ids = jnp.arange(N_EP, dtype=jnp.int32)[:, None]
    slot = (flat_ids * (N_EP * CAP) + group_ids * CAP + position).reshape(-1).astype(jnp.int32)
    sources = jnp.repeat(mid, TOP, axis=0)
    buffer = jnp.zeros((EXPERTS * N_EP * CAP, D), jnp.bfloat16).at[slot].set(sources)
    buffer = buffer.reshape(EXPERTS, N_EP * CAP, D)
    half_units = FE // N_TP

    def run_expert(items):
        rows_in, gate_w, up_w, down_w = items
        hidden = (jax.nn.silu(jnp.dot(rows_in, gate_w, preferred_element_type=jnp.float32)) * jnp.dot(rows_in, up_w, preferred_element_type=jnp.float32)).astype(jnp.bfloat16)
        total = jnp.zeros((rows_in.shape[0], D), jnp.float32)
        for part_idx in range(N_TP):
            lower = part_idx * half_units
            total = total + rounded(jnp.dot(hidden[:, lower:lower + half_units], down_w[lower:lower + half_units], preferred_element_type=jnp.float32))
        return total.astype(jnp.bfloat16)
    outputs = lax.map(run_expert, (buffer, expert_gate, expert_up, expert_down)).reshape(-1, D)
    picked = outputs[slot].astype(jnp.float32).reshape(BATCH, TOP, D)
    share = route_weights / lax.optimization_barrier(jnp.sum(route_weights, axis=1, keepdims=True)) * 2.5
    routed = lax.optimization_barrier(jnp.sum(share[..., None] * picked, axis=1))
    dense_hidden = (jax.nn.silu(jnp.dot(mid, dense_gate, preferred_element_type=jnp.float32)) * jnp.dot(mid, dense_up, preferred_element_type=jnp.float32)).astype(jnp.bfloat16)
    dense_out = jnp.dot(dense_hidden, dense_down, preferred_element_type=jnp.float32)
    mixed = (resid + routed + blend[:, None] * dense_out).astype(jnp.bfloat16)
    return (mixed, new_state)
```

```python
import jax
import jax.numpy as jnp
from jax import lax
from jax.sharding import PartitionSpec as P

BF = jnp.bfloat16
F32 = jnp.float32


def rms_norm(values, gain):
    scale = lax.rsqrt(jnp.mean(values * values, axis=-1, keepdims=True) + 1e-06)
    return values * scale * gain


def mixer_core(
    normed,
    prior_state,
    query_weight,
    key_weight,
    value_weight,
    decay_down,
    decay_up,
    decay_base,
    rate_down,
    rate_up,
    rate_base,
    head_gain,
):
    rows = normed.shape[0]
    heads_here = prior_state.shape[1]
    head_size = prior_state.shape[2]

    def project(weight):
        product = jnp.dot(normed, weight, preferred_element_type=F32).astype(BF).astype(F32)
        return product.reshape(rows, heads_here, head_size)

    receptance = project(query_weight)
    key_vec = project(key_weight)
    value_vec = project(value_weight)
    decay_low = jnp.tanh(jnp.dot(normed, decay_down, preferred_element_type=F32)).astype(BF)
    decay_log = decay_base + jnp.dot(decay_low, decay_up, preferred_element_type=F32)
    decay_log = -jax.nn.softplus(-decay_log) - 0.5
    decay_rate = jnp.exp(-jnp.exp(decay_log)).reshape(rows, heads_here, head_size)
    rate_low = jnp.dot(normed, rate_down, preferred_element_type=F32).astype(BF)
    learn_rate = jax.nn.sigmoid(rate_base + jnp.dot(rate_low, rate_up, preferred_element_type=F32))
    learn_rate = learn_rate.reshape(rows, heads_here, head_size)
    unit_key = key_vec * lax.rsqrt(jnp.sum(key_vec * key_vec, axis=-1, keepdims=True) + 1e-06)
    removed = jnp.sum(prior_state * unit_key[:, :, None, :], axis=-1)
    new_state = (
        prior_state * decay_rate[:, :, None, :]
        - removed[..., None] * (unit_key * learn_rate)[:, :, None, :]
        + value_vec[..., None] * key_vec[:, :, None, :]
    )
    read = jnp.sum(new_state * receptance[:, :, None, :], axis=-1)
    center = jnp.mean(read, axis=-1, keepdims=True)
    spread = jnp.mean(jnp.square(read - center), axis=-1, keepdims=True)
    normal = (read - center) * lax.rsqrt(spread + 0.00064)
    mixed_heads = (normal.reshape(rows, -1) * head_gain).astype(BF)
    return (mixed_heads, new_state)


def swap_tp(x):
    count = lax.axis_size("tp")
    return lax.ppermute(x, "tp", [(i, i ^ 1) for i in range(count)])


def swap_ep(x, mask):
    count = lax.axis_size("ep")
    return lax.ppermute(x, "ep", [(i, i ^ mask) for i in range(count)])


def shards(
    tokens,
    prior_state,
    first_gain,
    query_weight,
    key_weight,
    value_weight,
    decay_down,
    decay_up,
    decay_base,
    rate_down,
    rate_up,
    rate_base,
    head_gain,
    out_weight,
    mid_gain,
    route_ids,
    route_weights,
    expert_gate,
    expert_up,
    expert_down,
    dense_gate,
    dense_up,
    dense_down,
    blend_vector,
):
    count_ep = lax.axis_size("ep")
    seqs = tokens.shape[0]
    width = tokens.shape[1]
    top_count = route_ids.shape[1]
    half_width = width // 2
    token_f = tokens.astype(F32)
    normed = rms_norm(token_f, first_gain).astype(BF)
    mixed_heads, new_state = mixer_core(
        normed,
        prior_state,
        query_weight,
        key_weight,
        value_weight,
        decay_down,
        decay_up,
        decay_base,
        rate_down,
        rate_up,
        rate_base,
        head_gain,
    )
    partial_value = jnp.dot(mixed_heads, out_weight, preferred_element_type=F32).astype(BF)
    attn = partial_value.astype(F32) + swap_tp(partial_value).astype(F32)
    resid = (token_f + attn).astype(BF).astype(F32)
    mid = rms_norm(resid, mid_gain).astype(BF)
    blend = jax.nn.sigmoid(jnp.dot(mid, blend_vector, preferred_element_type=F32))

    share = route_weights / jnp.sum(route_weights, axis=1, keepdims=True) * 2.5
    scalars = jnp.concatenate([share, blend[:, None]], axis=1)
    upper = scalars.astype(BF)
    lower = (scalars - upper.astype(F32)).astype(BF)
    extra = jnp.concatenate([route_ids.astype(BF), upper, lower], axis=1)
    extra = jnp.pad(extra, ((0, 0), (0, 128 - extra.shape[1])))
    block = jnp.concatenate([mid, extra], axis=1)

    mask = count_ep // 2
    masks = []
    while mask >= 4:
        block = jnp.concatenate([block, swap_ep(block, mask)], axis=0)
        masks.append(mask)
        mask //= 2
    low = [m for m in range(1, 4) if m < count_ep]
    block = jnp.concatenate([block] + [swap_ep(block, m) for m in low], axis=0)
    rows = block.shape[0]

    piece = block[:, :width]
    info = block[:, width:].astype(F32)
    ids = info[:, :top_count]
    scalars = info[:, top_count : 2 * top_count + 1] + info[:, 2 * top_count + 1 : 3 * top_count + 2]
    here = lax.axis_index("ep").astype(F32)
    expert_scale = jnp.sum(jnp.where(ids == here, scalars[:, :top_count], 0.0), axis=1, keepdims=True)
    blend_scale = scalars[:, top_count :]

    def hidden(gate, up, scale):
        value = jax.nn.silu(jnp.dot(piece, gate, preferred_element_type=F32))
        return (value * jnp.dot(piece, up, preferred_element_type=F32) * scale).astype(BF)

    term = jnp.dot(
        hidden(expert_gate[0], expert_up[0], expert_scale), expert_down[0], preferred_element_type=F32
    ) + jnp.dot(hidden(dense_gate, dense_up, blend_scale), dense_down, preferred_element_type=F32)

    column = lax.axis_index("tp") * half_width
    mine = lax.dynamic_slice_in_dim(term, column, half_width, 1)
    other = lax.dynamic_slice_in_dim(term, half_width - column, half_width, 1).astype(BF)
    total = mine + swap_tp(other).astype(F32)

    groups = len(low) + 1
    part = total.reshape((groups, rows // groups, half_width))
    send = part.astype(BF)
    total = part[0] + sum(swap_ep(send[m], m).astype(F32) for m in low)
    for mask in reversed(masks):
        part = total.reshape((2, -1, half_width))
        total = part[0] + swap_ep(part[1].astype(BF), mask).astype(F32)

    own_cols = lax.dynamic_slice_in_dim(resid, column, half_width, 1)
    mixed = (own_cols + total).astype(BF)
    return (mixed, new_state)


def solution(mesh):
    in_specs = (
        P("ep", None),
        P("ep", "tp", None, None),
        P(),
        P(None, "tp"),
        P(None, "tp"),
        P(None, "tp"),
        P(),
        P(None, "tp"),
        P("tp"),
        P(),
        P(None, "tp"),
        P("tp"),
        P("tp"),
        P("tp", None),
        P(),
        P("ep", None),
        P("ep", None),
        P("ep", None, "tp"),
        P("ep", None, "tp"),
        P("ep", "tp", None),
        P(None, ("ep", "tp")),
        P(None, ("ep", "tp")),
        P(("ep", "tp"), None),
        P(),
    )
    out_specs = (P("ep", "tp"), P("ep", "tp", None, None))
    return jax.shard_map(shards, mesh=mesh, in_specs=in_specs, out_specs=out_specs, check_vma=False)
```

```python
import jax
import jax.numpy as jnp
from jax import lax
from jax.experimental import pallas as pl
from jax.experimental.pallas import tpu as pltpu
from jax.sharding import PartitionSpec as P

BF = jnp.bfloat16
F32 = jnp.float32
MIB = 1024 * 1024


VMEM = pl.BlockSpec(memory_space=pltpu.VMEM)
SMEM = pl.BlockSpec(memory_space=pltpu.SMEM)
HBM = pl.BlockSpec(memory_space=pltpu.MemorySpace.HBM)


def dot(a, b):
    return jnp.dot(a, b, preferred_element_type=F32)


def dot_nt(a, b):
    return lax.dot_general(a, b, (((1,), (1,)), ((), ())), preferred_element_type=F32)


def split(x):
    upper = x.astype(BF)
    return upper, (x - upper.astype(F32)).astype(BF)


def rms_norm(values, gain):
    scale = lax.rsqrt(jnp.mean(values * values, axis=-1, keepdims=True) + 1e-06)
    return values * scale * gain


def mixer_body(heads, head_size, *refs):
    count = 14
    sources, (partial_ref, aux_ref), scratch = refs[:count], refs[count : count + 2], refs[count + 2 :]
    places, sems = scratch[:count], scratch[count]
    copies = []
    for at in range(count - 1):
        copies.append(pltpu.make_async_copy(sources[at], places[at], sems.at[at]))
    state_src, state = sources[count - 1], places[count - 1]
    state_copies = [
        pltpu.make_async_copy(state_src.at[:, h], state.at[h], sems.at[count - 1 + h]) for h in range(heads)
    ]
    (tokens, gain, key_w, query_w, value_w, decay_down, rate_down, decay_up, rate_up, decay_base,
     rate_base, head_gain, out_w) = places[: count - 1]
    order = list(range(count - 2))
    for at in order:
        copies[at].start()
    for copy in state_copies:
        copy.start()
    copies[count - 2].start()

    seqs = tokens.shape[0]
    copies[0].wait()
    copies[1].wait()
    normed = rms_norm(tokens[...].astype(F32), gain[...]).astype(BF)
    copies[2].wait()
    key = dot(normed, key_w[...]).astype(BF)
    copies[3].wait()
    query = dot(normed, query_w[...]).astype(BF).astype(F32)
    copies[4].wait()
    value = dot(normed, value_w[...]).astype(BF).astype(F32)
    for at in range(5, count - 2):
        copies[at].wait()
    decay_low = jnp.tanh(dot_nt(normed, decay_down[...])).astype(BF)
    decay_log = decay_base[...] + dot(decay_low, decay_up[...])
    decay = jnp.exp(-jnp.exp(-0.5) / (1.0 + jnp.exp(-decay_log)))
    rate_low = dot_nt(normed, rate_down[...]).astype(BF)
    rate = 1.0 / (1.0 + jnp.exp(-(rate_base[...] + dot(rate_low, rate_up[...]))))
    read_key = decay * query
    read_upper, read_lower = split(read_key)
    key_f = key.astype(F32)

    cols = seqs * head_size
    row = lax.broadcasted_iota(jnp.int32, (seqs, cols), 0)
    lane = lax.broadcasted_iota(jnp.int32, (seqs, cols), 1)
    own = lane // head_size == row

    def fold(x):
        x = jnp.where(own, x, 0.0)
        while x.shape[1] > 2 * head_size:
            half = x.shape[1] // 2
            x = x[:, :half] + x[:, half:]
        return x[:, :head_size] + x[:, head_size:]

    pieces = []
    for h in range(heads):
        cut = slice(h * head_size, (h + 1) * head_size)
        key_h, query_h, value_h, decay_h = key_f[:, cut], query[:, cut], value[:, cut], decay[:, cut]
        rows = jnp.concatenate([key[:, cut], read_upper[:, cut], read_lower[:, cut]], axis=0)
        norm = lax.rsqrt(jnp.sum(key_h * key_h, axis=-1, keepdims=True) + 1e-06)
        unit = key_h * norm
        unit_rate = unit * rate[:, cut]
        state_copies[h].wait()
        upper, lower = split(state[h].reshape(cols, head_size))
        both = dot_nt(rows, upper) + dot_nt(rows, lower)
        removed = fold(both[:seqs]) * norm
        kept = fold(both[seqs : 2 * seqs] + both[2 * seqs :])
        read = (
            kept
            - removed * jnp.sum(unit_rate * query_h, axis=-1, keepdims=True)
            + value_h * jnp.sum(key_h * query_h, axis=-1, keepdims=True)
        )
        read = read - jnp.mean(read, axis=-1, keepdims=True)
        read = read * lax.rsqrt(jnp.mean(read * read, axis=-1, keepdims=True) + 0.00064)
        pieces.append(read)
        aux_ref[h, 0] = removed
        aux_ref[h, 1] = unit_rate
        aux_ref[h, 2] = decay_h
        aux_ref[h, 3] = key_h
        aux_ref[h, 4] = value_h
    mixed = (jnp.concatenate(pieces, axis=1) * head_gain[...]).astype(BF)
    copies[count - 2].wait()
    partial_ref[...] = dot(mixed, out_w[...]).astype(BF)


def mixer(tokens, gain, key_w, query_w, value_w, decay_down, rate_down, decay_up, rate_up, decay_base,
          rate_base, head_gain, out_w, state):
    seqs, heads, head_size = state.shape[0], state.shape[1], state.shape[3]
    args = (tokens, gain, key_w, query_w, value_w, decay_down, rate_down, decay_up, rate_up, decay_base,
            rate_base, head_gain, out_w, state)
    scratch = [pltpu.VMEM(a.shape, a.dtype) for a in args[:-1]]
    scratch.append(pltpu.VMEM((heads, seqs, head_size, head_size), F32))
    scratch.append(pltpu.SemaphoreType.DMA((len(args) + heads,)))
    return pl.pallas_call(
        lambda *refs: mixer_body(heads, head_size, *refs),
        out_shape=(
            jax.ShapeDtypeStruct((seqs, out_w.shape[1]), BF),
            jax.ShapeDtypeStruct((heads, 5, seqs, head_size), F32),
        ),
        in_specs=[HBM] * len(args),
        out_specs=(VMEM, VMEM),
        scratch_shapes=scratch,
        compiler_params=pltpu.CompilerParams(vmem_limit_bytes=16 * MIB),
        name="mixer",
    )(*(pltpu.with_memory_space_constraint(a, pltpu.MemorySpace.HBM) for a in args))


def state_body(state_ref, aux_ref, new_ref):
    seqs, _, size, _ = state_ref.shape
    cols = seqs * size
    removed, unit_rate, decay, key, value = (aux_ref[0, i] for i in range(5))
    removed_upper, removed_lower = (x.astype(F32) for x in split(removed))
    rate_upper, rate_lower = split(-unit_rate)
    left = jnp.concatenate([removed_upper, removed_lower, removed_upper, value], axis=0)
    right = jnp.concatenate([rate_upper, rate_upper, rate_lower, key.astype(BF)], axis=0)
    row = lax.broadcasted_iota(jnp.int32, (4 * seqs, cols), 0)
    lane = lax.broadcasted_iota(jnp.int32, (4 * seqs, cols), 1)
    left = jnp.where(lane // size == row % seqs, jnp.concatenate([left] * seqs, axis=1), 0.0)
    outer = dot(left.T.astype(BF), right)
    new_ref[:, 0] = state_ref[:, 0] * decay[:, None, :] + outer.reshape(seqs, size, size)


def update_state(state, aux):
    seqs, heads, size, _ = state.shape
    block = pl.BlockSpec((seqs, 1, size, size), lambda h: (0, h, 0, 0))
    return pl.pallas_call(
        state_body,
        grid=(heads,),
        out_shape=jax.ShapeDtypeStruct(state.shape, F32),
        in_specs=[block, pl.BlockSpec((1,) + aux.shape[1:], lambda h: (h, 0, 0, 0))],
        out_specs=block,
        cost_estimate=pl.CostEstimate(
            flops=4 * 64 * state.size, transcendentals=0, bytes_accessed=16 * state.size
        ),
        compiler_params=pltpu.CompilerParams(vmem_limit_bytes=16 * MIB),
        name="state_update",
    )(state, aux)


def ffn_body(pieces, top, half, *refs):
    place, places, blocks = refs[0], refs[1:7], refs[7 : 7 + pieces]
    other_ref, mine_ref = refs[7 + pieces : 9 + pieces]
    width = 2 * half
    rows = jnp.concatenate([b[:, :width] for b in blocks], axis=0)
    info = jnp.concatenate([b[:, width:] for b in blocks], axis=0).astype(F32)
    ids = info[:, :top]
    scalars = info[:, top : 2 * top + 1] + info[:, 2 * top + 1 : 3 * top + 2]
    here = place[0].astype(F32)
    scale = jnp.sum(jnp.where(ids == here, scalars[:, :top], 0.0), axis=1, keepdims=True)

    def hidden(at, by):
        gate = dot_nt(rows, places[at][...])
        up = dot_nt(rows, places[at + 1][...])
        return (gate / (1.0 + jnp.exp(-gate)) * up * by).astype(BF)

    expert = hidden(0, scale)
    dense = hidden(2, scalars[:, top:])
    column = pl.multiple_of(place[1] * half, 128)
    back = pl.multiple_of(half - column, 128)
    cut = (slice(None), pl.ds(back, half))
    other_ref[...] = (dot(expert, places[4][cut]) + dot(dense, places[5][cut])).astype(BF)
    cut = (slice(None), pl.ds(column, half))
    mine_ref[...] = dot(expert, places[4][cut]) + dot(dense, places[5][cut])


def ffn(place, weights, blocks, top):
    rows = sum(b.shape[0] for b in blocks)
    half = weights[-1].shape[1] // 2
    return pl.pallas_call(
        lambda *refs: ffn_body(len(blocks), top, half, *refs),
        out_shape=(jax.ShapeDtypeStruct((rows, half), BF), jax.ShapeDtypeStruct((rows, half), F32)),
        in_specs=[SMEM] + [VMEM] * (len(weights) + len(blocks)),
        out_specs=(VMEM, VMEM),
        compiler_params=pltpu.CompilerParams(vmem_limit_bytes=8 * MIB + rows * 22 * 1024),
        name="ffn",
    )(place, *weights, *blocks)


def swap_tp(x):
    count = lax.axis_size("tp")
    return lax.ppermute(x, "tp", [(i, i ^ 1) for i in range(count)])


def swap_ep(x, mask):
    count = lax.axis_size("ep")
    return lax.ppermute(x, "ep", [(i, i ^ mask) for i in range(count)])


def shards(
    tokens,
    prior_state,
    first_gain,
    query_weight,
    key_weight,
    value_weight,
    decay_down,
    decay_up,
    decay_base,
    rate_down,
    rate_up,
    rate_base,
    head_gain,
    out_weight,
    mid_gain,
    route_ids,
    route_weights,
    expert_gate,
    expert_up,
    expert_down,
    dense_gate,
    dense_up,
    dense_down,
    blend_vector,
):
    count_ep = lax.axis_size("ep")
    seqs = tokens.shape[0]
    width = tokens.shape[1]
    top_count = route_ids.shape[1]
    half_width = width // 2
    token_f = tokens.astype(F32)
    partial_value, aux = mixer(
        tokens,
        first_gain,
        key_weight,
        query_weight,
        value_weight,
        decay_down.T,
        rate_down.T,
        decay_up,
        rate_up,
        decay_base,
        rate_base,
        head_gain,
        out_weight,
        prior_state,
    )
    attn = partial_value.astype(F32) + swap_tp(partial_value).astype(F32)
    resid = (token_f + attn).astype(BF).astype(F32)
    mid = rms_norm(resid, mid_gain).astype(BF)
    blend = jax.nn.sigmoid(jnp.dot(mid, blend_vector, preferred_element_type=F32))

    share = route_weights / jnp.sum(route_weights, axis=1, keepdims=True) * 2.5
    scalars = jnp.concatenate([share, blend[:, None]], axis=1)
    upper = scalars.astype(BF)
    lower = (scalars - upper.astype(F32)).astype(BF)
    extra = jnp.concatenate([route_ids.astype(BF), upper, lower], axis=1)
    extra = jnp.pad(extra, ((0, 0), (0, 128 - extra.shape[1])))
    block = jnp.concatenate([mid, extra], axis=1)

    mask = count_ep // 2
    masks = []
    while mask >= 4:
        block = jnp.concatenate([block, swap_ep(block, mask)], axis=0)
        masks.append(mask)
        mask //= 2
    low = [m for m in range(1, 4) if m < count_ep]
    block, aux = lax.optimization_barrier((block, aux))
    new_state = update_state(prior_state, aux)
    blocks = [block] + [swap_ep(block, m) for m in low]
    blocks, new_state = lax.optimization_barrier((blocks, new_state))
    rows = sum(b.shape[0] for b in blocks)

    place = jnp.stack([lax.axis_index("ep"), lax.axis_index("tp")]).astype(jnp.int32)
    weights = (
        expert_gate[0].T,
        expert_up[0].T,
        dense_gate.T,
        dense_up.T,
        expert_down[0],
        dense_down,
    )
    other, mine = ffn(place, weights, blocks, top_count)
    column = lax.axis_index("tp") * half_width
    total = mine + swap_tp(other).astype(F32)

    groups = len(low) + 1
    part = total.reshape((groups, rows // groups, half_width))
    send = part.astype(BF)
    total = part[0] + sum(swap_ep(send[m], m).astype(F32) for m in low)
    for mask in reversed(masks):
        part = total.reshape((2, -1, half_width))
        total = part[0] + swap_ep(part[1].astype(BF), mask).astype(F32)

    own_cols = lax.dynamic_slice_in_dim(resid, column, half_width, 1)
    mixed = (own_cols + total).astype(BF)
    return (mixed, new_state)


def solution(mesh):
    in_specs = (
        P("ep", None),
        P("ep", "tp", None, None),
        P(),
        P(None, "tp"),
        P(None, "tp"),
        P(None, "tp"),
        P(),
        P(None, "tp"),
        P("tp"),
        P(),
        P(None, "tp"),
        P("tp"),
        P("tp"),
        P("tp", None),
        P(),
        P("ep", None),
        P("ep", None),
        P("ep", None, "tp"),
        P("ep", None, "tp"),
        P("ep", "tp", None),
        P(None, ("ep", "tp")),
        P(None, ("ep", "tp")),
        P(("ep", "tp"), None),
        P(),
    )
    out_specs = (P("ep", "tp"), P("ep", "tp", None, None))
    return jax.shard_map(shards, mesh=mesh, in_specs=in_specs, out_specs=out_specs, check_vma=False)
```

```python
import jax
import jax.numpy as jnp
from jax import lax
from jax.experimental import pallas as pl
from jax.experimental.pallas import tpu as pltpu
from jax.sharding import PartitionSpec as P

BF = jnp.bfloat16
F32 = jnp.float32
MIB = 1024 * 1024


VMEM = pl.BlockSpec(memory_space=pltpu.VMEM)
HBM = pl.BlockSpec(memory_space=pltpu.MemorySpace.HBM)


def in_hbm(x):
    return pltpu.with_memory_space_constraint(x, pltpu.MemorySpace.HBM)


def dot(a, b):
    return jnp.dot(a, b, preferred_element_type=F32)


def dot_nt(a, b):
    return lax.dot_general(a, b, (((1,), (1,)), ((), ())), preferred_element_type=F32)


def split(x):
    upper = x.astype(BF)
    return upper, (x - upper.astype(F32)).astype(BF)


def rms_norm(values, gain):
    scale = lax.rsqrt(jnp.mean(values * values, axis=-1, keepdims=True) + 1e-06)
    return values * scale * gain


def mixer_body(heads, head_size, *refs):
    count = 16
    sources, (partial_ref, base_ref, aux_ref, extra_ref) = refs[:count], refs[count : count + 4]
    places, sems = refs[count + 4 : 2 * count + 4], refs[2 * count + 4]
    copies = [pltpu.make_async_copy(sources[at], places[at], sems.at[at]) for at in range(count - 1)]
    state_src, state = sources[count - 1], places[count - 1]
    state_copies = [
        pltpu.make_async_copy(state_src.at[:, h], state.at[h], sems.at[count - 1 + h]) for h in range(heads)
    ]
    (tokens, gain, route_ids, route_weights, key_w, query_w, value_w, decay_down, rate_down, decay_up,
     rate_up, decay_base, rate_base, head_gain, out_w) = places[: count - 1]
    for copy in copies[: count - 2] + state_copies + copies[count - 2 :]:
        copy.start()

    for at in range(2, 4):
        copies[at].wait()
    weights = route_weights[...]
    share = weights / jnp.sum(weights, axis=0, keepdims=True) * 2.5
    upper = share.astype(BF).astype(F32)
    info = jnp.concatenate([route_ids[...].astype(F32), upper, share - upper], axis=0)
    lanes = extra_ref.shape[1]
    info = jnp.concatenate([info, jnp.zeros((lanes - info.shape[0], info.shape[1]), F32)], axis=0)
    extra_ref[...] = info.T.astype(BF)

    seqs = tokens.shape[0]
    copies[0].wait()
    copies[1].wait()
    normed = rms_norm(tokens[...].astype(F32), gain[...]).astype(BF)
    copies[4].wait()
    key = dot(normed, key_w[...]).astype(BF)
    copies[5].wait()
    query = dot(normed, query_w[...]).astype(BF).astype(F32)
    copies[6].wait()
    value = dot(normed, value_w[...]).astype(BF).astype(F32)
    for at in range(7, count - 2):
        copies[at].wait()
    decay_low = jnp.tanh(dot_nt(normed, decay_down[...])).astype(BF)
    decay_log = decay_base[...] + dot(decay_low, decay_up[...])
    decay = jnp.exp(-jnp.exp(-0.5) / (1.0 + jnp.exp(-decay_log)))
    rate_low = dot_nt(normed, rate_down[...]).astype(BF)
    rate = 1.0 / (1.0 + jnp.exp(-(rate_base[...] + dot(rate_low, rate_up[...]))))
    read_key = decay * query
    read_upper, read_lower = split(read_key)
    key_f = key.astype(F32)

    cols = seqs * head_size
    row = lax.broadcasted_iota(jnp.int32, (seqs, cols), 0)
    lane = lax.broadcasted_iota(jnp.int32, (seqs, cols), 1)
    own = lane // head_size == row

    def fold(x):
        x = jnp.where(own, x, 0.0)
        while x.shape[1] > 2 * head_size:
            half = x.shape[1] // 2
            x = x[:, :half] + x[:, half:]
        return x[:, :head_size] + x[:, head_size:]

    pieces = []
    for h in range(heads):
        cut = slice(h * head_size, (h + 1) * head_size)
        key_h, query_h, value_h, decay_h = key_f[:, cut], query[:, cut], value[:, cut], decay[:, cut]
        rows = jnp.concatenate([key[:, cut], read_upper[:, cut], read_lower[:, cut]], axis=0)
        norm = lax.rsqrt(jnp.sum(key_h * key_h, axis=-1, keepdims=True) + 1e-06)
        unit = key_h * norm
        unit_rate = unit * rate[:, cut]
        state_copies[h].wait()
        upper, lower = split(state[h].reshape(cols, head_size))
        both = dot_nt(rows, upper) + dot_nt(rows, lower)
        removed = fold(both[:seqs]) * norm
        kept = fold(both[seqs : 2 * seqs] + both[2 * seqs :])
        read = (
            kept
            - removed * jnp.sum(unit_rate * query_h, axis=-1, keepdims=True)
            + value_h * jnp.sum(key_h * query_h, axis=-1, keepdims=True)
        )
        read = read - jnp.mean(read, axis=-1, keepdims=True)
        read = read * lax.rsqrt(jnp.mean(read * read, axis=-1, keepdims=True) + 0.00064)
        pieces.append(read)
        aux_ref[h, 0] = removed
        aux_ref[h, 1] = unit_rate
        aux_ref[h, 2] = decay_h
        aux_ref[h, 3] = key_h
        aux_ref[h, 4] = value_h
    mixed = (jnp.concatenate(pieces, axis=1) * head_gain[...]).astype(BF)
    copies[count - 2].wait()
    partial = dot(mixed, out_w[...]).astype(BF)
    partial_ref[...] = partial
    base_ref[...] = tokens[...].astype(F32) + partial.astype(F32)


def mixer(*args):
    seqs, heads, _, head_size = args[-1].shape
    width = args[0].shape[1]
    scratch = [pltpu.VMEM(a.shape, a.dtype) for a in args[:-1]]
    scratch.append(pltpu.VMEM((heads, seqs, head_size, head_size), F32))
    scratch.append(pltpu.SemaphoreType.DMA((len(args) + heads,)))
    return pl.pallas_call(
        lambda *refs: mixer_body(heads, head_size, *refs),
        out_shape=(
            pltpu.VMEM((seqs, width), BF),
            pltpu.VMEM((seqs, width), F32),
            pltpu.VMEM((heads, 5, seqs, head_size), F32),
            pltpu.VMEM((seqs, 128), BF),
        ),
        in_specs=[HBM] * len(args),
        out_specs=(VMEM,) * 4,
        scratch_shapes=scratch,
        compiler_params=pltpu.CompilerParams(vmem_limit_bytes=16 * MIB),
        name="mixer",
    )(*(in_hbm(a) for a in args))


def state_body(state_ref, aux_ref, new_ref):
    seqs, _, size, _ = state_ref.shape
    cols = seqs * size
    removed, unit_rate, decay, key, value = (aux_ref[pl.program_id(0), i] for i in range(5))
    removed_upper, removed_lower = (x.astype(F32) for x in split(removed))
    rate_upper, rate_lower = split(-unit_rate)
    left = jnp.concatenate([removed_upper, removed_lower, removed_upper, value], axis=0)
    right = jnp.concatenate([rate_upper, rate_upper, rate_lower, key.astype(BF)], axis=0)
    row = lax.broadcasted_iota(jnp.int32, (4 * seqs, cols), 0)
    lane = lax.broadcasted_iota(jnp.int32, (4 * seqs, cols), 1)
    left = jnp.where(lane // size == row % seqs, jnp.concatenate([left] * seqs, axis=1), 0.0)
    outer = dot(left.T.astype(BF), right)
    new_ref[:, 0] = state_ref[:, 0] * decay[:, None, :] + outer.reshape(seqs, size, size)


def update_state(state, aux):
    seqs, heads, size, _ = state.shape
    block = pl.BlockSpec((seqs, 1, size, size), lambda h: (0, h, 0, 0))
    return pl.pallas_call(
        state_body,
        grid=(heads,),
        out_shape=jax.ShapeDtypeStruct(state.shape, F32),
        in_specs=[block, VMEM],
        out_specs=block,
        cost_estimate=pl.CostEstimate(
            flops=4 * 64 * state.size, transcendentals=0, bytes_accessed=16 * state.size
        ),
        compiler_params=pltpu.CompilerParams(vmem_limit_bytes=16 * MIB),
        name="state_update",
    )(state, aux)


def pack_body(top, half, base, other, gain, blend_vector, extra, block_ref, resid_ref):
    resid = (base[...] + other[...].astype(F32)).astype(BF).astype(F32)
    mid = rms_norm(resid, gain[...]).astype(BF)
    score = jnp.sum(mid.astype(F32) * blend_vector[...].astype(F32), axis=-1, keepdims=True)
    upper, lower = (x.astype(F32) for x in split(1.0 / (1.0 + jnp.exp(-score))))
    info = extra[...].astype(F32)
    lane = lax.broadcasted_iota(jnp.int32, info.shape, 1)
    info = jnp.where(lane == 3 * top, upper, jnp.where(lane == 3 * top + 1, lower, info))
    first = lax.axis_index("tp") == 0
    block_ref[:, :half] = jnp.where(first, mid[:, :half], mid[:, half:])
    block_ref[:, half:] = info.astype(BF)
    resid_ref[...] = jnp.where(first, resid[:, :half], resid[:, half:])


def pack(base, other, gain, blend_vector, extra, top):
    seqs, width = base.shape
    half = width // 2
    return pl.pallas_call(
        lambda *refs: pack_body(top, half, *refs),
        out_shape=(
            pltpu.VMEM((seqs, half + extra.shape[1]), BF),
            pltpu.VMEM((seqs, half), F32),
        ),
        in_specs=[VMEM] * 5,
        out_specs=(VMEM, VMEM),
        compiler_params=pltpu.CompilerParams(vmem_limit_bytes=4 * MIB),
        name="pack",
    )(base, other, gain, blend_vector, extra)


def ffn_body(pieces, top, half, *refs):
    places, blocks = refs[:6], refs[6 : 6 + 2 * pieces]
    other_ref, mine_ref = refs[6 + 2 * pieces :]
    near = jnp.concatenate([b[:, :half] for b in blocks[:pieces]], axis=0)
    far = jnp.concatenate([b[:, :half] for b in blocks[pieces:]], axis=0)
    first = lax.axis_index("tp") == 0
    rows = jnp.concatenate([jnp.where(first, near, far), jnp.where(first, far, near)], axis=1)
    info = jnp.concatenate([b[:, half:] for b in blocks[:pieces]], axis=0).astype(F32)
    scalars = info[:, top : 2 * top] + info[:, 2 * top : 3 * top]
    here = lax.axis_index("ep").astype(F32)
    scale = jnp.sum(jnp.where(info[:, :top] == here, scalars, 0.0), axis=1, keepdims=True)
    blend = info[:, 3 * top : 3 * top + 1] + info[:, 3 * top + 1 : 3 * top + 2]

    def hidden(at, by):
        gate = dot_nt(rows, places[at][...])
        up = dot_nt(rows, places[at + 1][...])
        return (gate / (1.0 + jnp.exp(-gate)) * up * by).astype(BF)

    expert = hidden(0, scale)
    dense = hidden(2, blend)
    column = pl.multiple_of(lax.axis_index("tp") * half, 128)
    back = pl.multiple_of(half - column, 128)
    cut = (slice(None), pl.ds(back, half))
    other_ref[...] = (dot(expert, places[4][cut]) + dot(dense, places[5][cut])).astype(BF)
    cut = (slice(None), pl.ds(column, half))
    mine_ref[...] = dot(expert, places[4][cut]) + dot(dense, places[5][cut])


def ffn(weights, near, far, top):
    rows = sum(b.shape[0] for b in near)
    half = weights[-1].shape[1] // 2
    return pl.pallas_call(
        lambda *refs: ffn_body(len(near), top, half, *refs),
        out_shape=(pltpu.VMEM((rows, half), BF), pltpu.VMEM((rows, half), F32)),
        in_specs=[VMEM] * (len(weights) + 2 * len(near)),
        out_specs=(VMEM, VMEM),
        compiler_params=pltpu.CompilerParams(vmem_limit_bytes=8 * MIB + rows * 22 * 1024),
        name="ffn",
    )(*weights, *near, *far)


def swap_tp(x):
    count = lax.axis_size("tp")
    return lax.ppermute(x, "tp", [(i, i ^ 1) for i in range(count)])


def swap_ep(x, mask):
    count = lax.axis_size("ep")
    return lax.ppermute(x, "ep", [(i, i ^ mask) for i in range(count)])


def shards(
    tokens,
    prior_state,
    first_gain,
    query_weight,
    key_weight,
    value_weight,
    decay_down,
    decay_up,
    decay_base,
    rate_down,
    rate_up,
    rate_base,
    head_gain,
    out_weight,
    mid_gain,
    route_ids,
    route_weights,
    expert_gate,
    expert_up,
    expert_down,
    dense_gate,
    dense_up,
    dense_down,
    blend_vector,
):
    count_ep = lax.axis_size("ep")
    seqs = tokens.shape[0]
    width = tokens.shape[1]
    top_count = route_ids.shape[1]
    half_width = width // 2
    partial_value, base, aux, extra = mixer(
        tokens,
        first_gain,
        route_ids.T,
        route_weights.T,
        key_weight,
        query_weight,
        value_weight,
        decay_down.T,
        rate_down.T,
        decay_up,
        rate_up,
        decay_base,
        rate_base,
        head_gain,
        out_weight,
        prior_state,
    )
    block, resid = pack(base, swap_tp(partial_value), mid_gain, blend_vector, extra, top_count)

    mask = count_ep // 2
    masks = []
    while mask >= 4:
        block = jnp.concatenate([block, swap_ep(block, mask)], axis=0)
        masks.append(mask)
        mask //= 2
    low = [m for m in (1, 3, 2) if m < count_ep]
    near = [block] + [swap_ep(block, m) for m in low]
    far = [swap_tp(b) for b in near]
    rows = sum(b.shape[0] for b in near)

    weights = (
        expert_gate[0].T,
        expert_up[0].T,
        dense_gate.T,
        dense_up.T,
        expert_down[0],
        dense_down,
    )
    other, mine = ffn(weights, near, far, top_count)
    total = mine + swap_tp(other).astype(F32)

    groups = len(low) + 1
    part = total.reshape((groups, rows // groups, half_width))
    send, aux = lax.optimization_barrier((part.astype(BF), aux))
    new_state = update_state(prior_state, aux)
    back = [swap_ep(send[i + 1], m) for i, m in enumerate(low)]
    back, new_state = lax.optimization_barrier((back, new_state))
    total = part[0] + sum(x.astype(F32) for x in back)
    for mask in reversed(masks):
        part = total.reshape((2, -1, half_width))
        total = part[0] + swap_ep(part[1].astype(BF), mask).astype(F32)

    mixed = (resid + total).astype(BF)
    return (mixed, new_state)


def solution(mesh):
    in_specs = (
        P("ep", None),
        P("ep", "tp", None, None),
        P(),
        P(None, "tp"),
        P(None, "tp"),
        P(None, "tp"),
        P(),
        P(None, "tp"),
        P("tp"),
        P(),
        P(None, "tp"),
        P("tp"),
        P("tp"),
        P("tp", None),
        P(),
        P("ep", None),
        P("ep", None),
        P("ep", None, "tp"),
        P("ep", None, "tp"),
        P("ep", "tp", None),
        P(None, ("ep", "tp")),
        P(None, ("ep", "tp")),
        P(("ep", "tp"), None),
        P(),
    )
    out_specs = (P("ep", "tp"), P("ep", "tp", None, None))
    return jax.shard_map(shards, mesh=mesh, in_specs=in_specs, out_specs=out_specs, check_vma=False)
```

```python
import jax
import jax.numpy as jnp
from jax import lax
from jax.experimental import pallas as pl
from jax.experimental.pallas import tpu as pltpu
from jax.sharding import PartitionSpec as P

BF = jnp.bfloat16
F32 = jnp.float32
MIB = 1024 * 1024


VMEM = pl.BlockSpec(memory_space=pltpu.VMEM)
HBM = pl.BlockSpec(memory_space=pltpu.MemorySpace.HBM)


def in_hbm(x):
    return pltpu.with_memory_space_constraint(x, pltpu.MemorySpace.HBM)


def dot(a, b):
    return jnp.dot(a, b, preferred_element_type=F32)


def dot_nt(a, b):
    return lax.dot_general(a, b, (((1,), (1,)), ((), ())), preferred_element_type=F32)


def split(x):
    upper = x.astype(BF)
    return upper, (x - upper.astype(F32)).astype(BF)


def rms_norm(values, gain):
    scale = lax.rsqrt(jnp.mean(values * values, axis=-1, keepdims=True) + 1e-06)
    return values * scale * gain


def mixer_body(heads, head_size, *refs):
    count = 16
    sources, (partial_ref, base_ref, aux_ref, extra_ref) = refs[:count], refs[count : count + 4]
    places, sems = refs[count + 4 : 2 * count + 4], refs[2 * count + 4]
    copies = [pltpu.make_async_copy(sources[at], places[at], sems.at[at]) for at in range(count - 1)]
    state_src, state = sources[count - 1], places[count - 1]
    state_copies = [
        pltpu.make_async_copy(state_src.at[:, h], state.at[h], sems.at[count - 1 + h]) for h in range(heads)
    ]
    (tokens, gain, route_ids, route_weights, key_w, query_w, value_w, decay_down, rate_down, decay_up,
     rate_up, decay_base, rate_base, head_gain, out_w) = places[: count - 1]
    for copy in copies[: count - 2] + state_copies + copies[count - 2 :]:
        copy.start()

    for at in range(2, 4):
        copies[at].wait()
    weights = route_weights[...]
    share = weights / jnp.sum(weights, axis=0, keepdims=True) * 2.5
    upper = share.astype(BF).astype(F32)
    info = jnp.concatenate([route_ids[...].astype(F32), upper, share - upper], axis=0)
    lanes = extra_ref.shape[1]
    info = jnp.concatenate([info, jnp.zeros((lanes - info.shape[0], info.shape[1]), F32)], axis=0)
    extra_ref[...] = info.T.astype(BF)

    seqs = tokens.shape[0]
    copies[0].wait()
    copies[1].wait()
    normed = rms_norm(tokens[...].astype(F32), gain[...]).astype(BF)
    copies[4].wait()
    key = dot(normed, key_w[...]).astype(BF).astype(F32)
    copies[5].wait()
    query = dot(normed, query_w[...]).astype(BF).astype(F32)
    copies[6].wait()
    value = dot(normed, value_w[...]).astype(BF).astype(F32)
    for at in range(7, count - 2):
        copies[at].wait()
    decay_low = jnp.tanh(dot_nt(normed, decay_down[...])).astype(BF)
    decay_log = decay_base[...] + dot(decay_low, decay_up[...])
    decay = jnp.exp(-jnp.exp(-0.5) / (1.0 + jnp.exp(-decay_log)))
    rate_low = dot_nt(normed, rate_down[...]).astype(BF)
    rate = 1.0 / (1.0 + jnp.exp(-(rate_base[...] + dot(rate_low, rate_up[...]))))

    def stacked(x):
        return jnp.concatenate([x[:, h * head_size : (h + 1) * head_size] for h in range(heads)], axis=0)

    def shared(x):
        return jnp.sum(x, axis=-1, keepdims=True)

    key, query, value, decay, rate = (stacked(x) for x in (key, query, value, decay, rate))
    read_upper, read_lower = split(decay * query)
    norm = lax.rsqrt(shared(key * key) + 1e-06)
    unit_rate = key * norm * rate
    removed_part = shared(unit_rate * query)
    value_part = shared(key * query)
    for at, x in ((1, unit_rate), (2, decay), (3, key), (4, value)):
        aux_ref[at] = x.reshape(heads, seqs, head_size)
    key = key.astype(BF)

    cols = seqs * head_size
    row = lax.broadcasted_iota(jnp.int32, (seqs, cols), 0)
    lane = lax.broadcasted_iota(jnp.int32, (seqs, cols), 1)
    own = lane // head_size == row

    def fold(x):
        x = jnp.where(own, x, 0.0)
        while x.shape[1] > 2 * head_size:
            half = x.shape[1] // 2
            x = x[:, :half] + x[:, half:]
        return x

    for copy in state_copies:
        copy.wait()
    removed, kept = [], []
    for h in range(heads):
        cut = slice(h * seqs, (h + 1) * seqs)
        rows = jnp.concatenate([key[cut], read_upper[cut], read_lower[cut]], axis=0)
        upper, lower = split(state[h].reshape(cols, head_size))
        both = dot_nt(rows, upper) + dot_nt(rows, lower)
        removed.append(fold(both[:seqs]))
        kept.append(fold(both[seqs : 2 * seqs] + both[2 * seqs :]))
    removed, kept = (jnp.concatenate(x, axis=0) for x in (removed, kept))
    removed = (removed[:, :head_size] + removed[:, head_size:]) * norm
    kept = kept[:, :head_size] + kept[:, head_size:]
    aux_ref[0] = removed.reshape(heads, seqs, head_size)
    read = kept - removed * removed_part + value * value_part
    read = read - jnp.mean(read, axis=-1, keepdims=True)
    read = read * lax.rsqrt(jnp.mean(read * read, axis=-1, keepdims=True) + 0.00064)
    pieces = [read[h * seqs : (h + 1) * seqs] for h in range(heads)]
    mixed = (jnp.concatenate(pieces, axis=1) * head_gain[...]).astype(BF)
    copies[count - 2].wait()
    partial = dot(mixed, out_w[...]).astype(BF)
    partial_ref[...] = partial
    base_ref[...] = tokens[...].astype(F32) + partial.astype(F32)


def mixer(*args):
    seqs, heads, _, head_size = args[-1].shape
    width = args[0].shape[1]
    scratch = [pltpu.VMEM(a.shape, a.dtype) for a in args[:-1]]
    scratch.append(pltpu.VMEM((heads, seqs, head_size, head_size), F32))
    scratch.append(pltpu.SemaphoreType.DMA((len(args) + heads,)))
    return pl.pallas_call(
        lambda *refs: mixer_body(heads, head_size, *refs),
        out_shape=(
            pltpu.VMEM((seqs, width), BF),
            pltpu.VMEM((seqs, width), F32),
            pltpu.VMEM((5, heads, seqs, head_size), F32),
            pltpu.VMEM((seqs, 128), BF),
        ),
        in_specs=[HBM] * len(args),
        out_specs=(VMEM,) * 4,
        scratch_shapes=scratch,
        compiler_params=pltpu.CompilerParams(vmem_limit_bytes=16 * MIB),
        name="mixer",
    )(*(in_hbm(a) for a in args))


def state_body(state_ref, aux_ref, new_ref):
    seqs, _, size, _ = state_ref.shape
    cols = seqs * size
    removed, unit_rate, decay, key, value = (aux_ref[i, pl.program_id(0)] for i in range(5))
    removed_upper, removed_lower = (x.astype(F32) for x in split(removed))
    rate_upper, rate_lower = split(-unit_rate)
    left = jnp.concatenate([removed_upper, removed_lower, removed_upper, value], axis=0)
    right = jnp.concatenate([rate_upper, rate_upper, rate_lower, key.astype(BF)], axis=0)
    row = lax.broadcasted_iota(jnp.int32, (4 * seqs, cols), 0)
    lane = lax.broadcasted_iota(jnp.int32, (4 * seqs, cols), 1)
    left = jnp.where(lane // size == row % seqs, jnp.concatenate([left] * seqs, axis=1), 0.0)
    outer = dot(left.T.astype(BF), right)
    new_ref[:, 0] = state_ref[:, 0] * decay[:, None, :] + outer.reshape(seqs, size, size)


def update_state(state, aux):
    seqs, heads, size, _ = state.shape
    block = pl.BlockSpec((seqs, 1, size, size), lambda h: (0, h, 0, 0))
    return pl.pallas_call(
        state_body,
        grid=(heads,),
        out_shape=jax.ShapeDtypeStruct(state.shape, F32),
        in_specs=[block, VMEM],
        out_specs=block,
        cost_estimate=pl.CostEstimate(
            flops=4 * 64 * state.size, transcendentals=0, bytes_accessed=16 * state.size
        ),
        compiler_params=pltpu.CompilerParams(vmem_limit_bytes=16 * MIB),
        name="state_update",
    )(state, aux)


def pack_body(top, half, base, other, gain, blend_vector, extra, block_ref, resid_ref):
    resid = (base[...] + other[...].astype(F32)).astype(BF).astype(F32)
    mid = rms_norm(resid, gain[...]).astype(BF)
    score = jnp.sum(mid.astype(F32) * blend_vector[...].astype(F32), axis=-1, keepdims=True)
    upper, lower = (x.astype(F32) for x in split(1.0 / (1.0 + jnp.exp(-score))))
    info = extra[...].astype(F32)
    lane = lax.broadcasted_iota(jnp.int32, info.shape, 1)
    info = jnp.where(lane == 3 * top, upper, jnp.where(lane == 3 * top + 1, lower, info))
    first = lax.axis_index("tp") == 0
    block_ref[:, :half] = jnp.where(first, mid[:, :half], mid[:, half:])
    block_ref[:, half:] = info.astype(BF)
    resid_ref[...] = jnp.where(first, resid[:, :half], resid[:, half:])


def pack(base, other, gain, blend_vector, extra, top):
    seqs, width = base.shape
    half = width // 2
    return pl.pallas_call(
        lambda *refs: pack_body(top, half, *refs),
        out_shape=(
            pltpu.VMEM((seqs, half + extra.shape[1]), BF),
            pltpu.VMEM((seqs, half), F32),
        ),
        in_specs=[VMEM] * 5,
        out_specs=(VMEM, VMEM),
        compiler_params=pltpu.CompilerParams(vmem_limit_bytes=4 * MIB),
        name="pack",
    )(base, other, gain, blend_vector, extra)


def ffn_body(pieces, seqs, top, half, *refs):
    places, blocks = refs[:6], refs[6 : 6 + 2 * pieces]
    other_ref, mine_ref = refs[6 + 2 * pieces :]
    near = jnp.concatenate([b[:, :half] for b in blocks[:pieces]], axis=0)
    far = jnp.concatenate([b[:, :half] for b in blocks[pieces:]], axis=0)
    first = lax.axis_index("tp") == 0
    rows = jnp.concatenate([jnp.where(first, near, far), jnp.where(first, far, near)], axis=1)
    info = jnp.concatenate([b[:, half:] for b in blocks[:pieces]], axis=0).astype(F32)
    scalars = info[:, top : 2 * top] + info[:, 2 * top : 3 * top]
    here = lax.axis_index("ep").astype(F32)
    scale = jnp.sum(jnp.where(info[:, :top] == here, scalars, 0.0), axis=1, keepdims=True)
    blend = info[:, 3 * top : 3 * top + 1] + info[:, 3 * top + 1 : 3 * top + 2]

    def hidden(at, by):
        gate = dot_nt(rows, places[at][...])
        up = dot_nt(rows, places[at + 1][...])
        return (gate / (1.0 + jnp.exp(-gate)) * up * by).astype(BF)

    expert = hidden(0, scale)
    dense = hidden(2, blend)
    count = blocks[0].shape[0] // seqs
    chunk = lax.broadcasted_iota(jnp.int32, (near.shape[0], 1), 0) // seqs % count
    side = chunk * 0 + lax.axis_index("tp")
    for bit in range(count.bit_length() - 1):
        side = side ^ (chunk >> bit & 1)
    low = dot(expert, places[4][:, :half]) + dot(dense, places[5][:, :half])
    high = dot(expert, places[4][:, half:]) + dot(dense, places[5][:, half:])
    other_ref[...] = jnp.where(side == 0, high, low).astype(BF)
    mine_ref[...] = jnp.where(side == 0, low, high)


def ffn(weights, near, far, seqs, top):
    rows = sum(b.shape[0] for b in near)
    half = weights[-1].shape[1] // 2
    return pl.pallas_call(
        lambda *refs: ffn_body(len(near), seqs, top, half, *refs),
        out_shape=(pltpu.VMEM((rows, half), BF), pltpu.VMEM((rows, half), F32)),
        in_specs=[VMEM] * (len(weights) + 2 * len(near)),
        out_specs=(VMEM, VMEM),
        compiler_params=pltpu.CompilerParams(vmem_limit_bytes=8 * MIB + rows * 20 * 1024),
        name="ffn",
    )(*weights, *near, *far)


def swap_tp(x):
    count = lax.axis_size("tp")
    return lax.ppermute(x, "tp", [(i, i ^ 1) for i in range(count)])


def cross(x, mask):
    size = lax.axis_size("tp")
    pairs = [
        (i * size + j, (i ^ mask) * size + (j ^ 1)) for i in range(lax.axis_size("ep")) for j in range(size)
    ]
    return lax.ppermute(x, ("ep", "tp"), pairs)


def swap_ep(x, mask):
    count = lax.axis_size("ep")
    return lax.ppermute(x, "ep", [(i, i ^ mask) for i in range(count)])


def shards(
    tokens,
    prior_state,
    first_gain,
    query_weight,
    key_weight,
    value_weight,
    decay_down,
    decay_up,
    decay_base,
    rate_down,
    rate_up,
    rate_base,
    head_gain,
    out_weight,
    mid_gain,
    route_ids,
    route_weights,
    expert_gate,
    expert_up,
    expert_down,
    dense_gate,
    dense_up,
    dense_down,
    blend_vector,
):
    count_ep = lax.axis_size("ep")
    seqs = tokens.shape[0]
    width = tokens.shape[1]
    top_count = route_ids.shape[1]
    half_width = width // 2
    partial_value, base, aux, extra = mixer(
        tokens,
        first_gain,
        route_ids.T,
        route_weights.T,
        key_weight,
        query_weight,
        value_weight,
        decay_down.T,
        rate_down.T,
        decay_up,
        rate_up,
        decay_base,
        rate_base,
        head_gain,
        out_weight,
        prior_state,
    )
    block, resid = pack(base, swap_tp(partial_value), mid_gain, blend_vector, extra, top_count)

    mask = count_ep // 2
    masks = []
    while mask >= 4:
        block = jnp.concatenate([block, swap_ep(block, mask)], axis=0)
        masks.append(mask)
        mask //= 2
    low = [m for m in (1, 3, 2) if m < count_ep]
    near = [block] + [swap_ep(block, m) for m in low]
    far = [swap_tp(b) for b in near]
    rows = sum(b.shape[0] for b in near)

    weights = (
        expert_gate[0].T,
        expert_up[0].T,
        dense_gate.T,
        dense_up.T,
        expert_down[0],
        dense_down,
    )
    other, mine = ffn(weights, near, far, seqs, top_count)
    total = mine + swap_tp(other).astype(F32)

    groups = len(low) + 1
    part = total.reshape((groups, rows // groups, half_width))
    send, aux = lax.optimization_barrier((part.astype(BF), aux))
    new_state = update_state(prior_state, aux)
    back = [swap_ep(send[i + 1], m) for i, m in enumerate(low)]
    back, new_state = lax.optimization_barrier((back, new_state))
    total = part[0] + sum(x.astype(F32) for x in back)
    for mask in reversed(masks):
        part = total.reshape((2, -1, half_width))
        total = part[0] + cross(part[1].astype(BF), mask).astype(F32)

    mixed = (resid + total).astype(BF)
    return (mixed, new_state)


def solution(mesh):
    in_specs = (
        P("ep", None),
        P("ep", "tp", None, None),
        P(),
        P(None, "tp"),
        P(None, "tp"),
        P(None, "tp"),
        P(),
        P(None, "tp"),
        P("tp"),
        P(),
        P(None, "tp"),
        P("tp"),
        P("tp"),
        P("tp", None),
        P(),
        P("ep", None),
        P("ep", None),
        P("ep", None, "tp"),
        P("ep", None, "tp"),
        P("ep", "tp", None),
        P(None, ("ep", "tp")),
        P(None, ("ep", "tp")),
        P(("ep", "tp"), None),
        P(),
    )
    out_specs = (P("ep", "tp"), P("ep", "tp", None, None))
    return jax.shard_map(shards, mesh=mesh, in_specs=in_specs, out_specs=out_specs, check_vma=False)
```

```python
import jax
import jax.numpy as jnp
from jax import lax
from jax.experimental import pallas as pl
from jax.experimental.pallas import tpu as pltpu
from jax.sharding import PartitionSpec as P

BF = jnp.bfloat16
F32 = jnp.float32
MIB = 1024 * 1024
GATHER_TURNS = (3, 1, 2)
REDUCE_TURNS = (3, 2, 1)


VMEM = pl.BlockSpec(memory_space=pltpu.VMEM)
HBM = pl.BlockSpec(memory_space=pltpu.MemorySpace.HBM)


def in_hbm(x):
    return pltpu.with_memory_space_constraint(x, pltpu.MemorySpace.HBM)


def dot(a, b):
    return jnp.dot(a, b, preferred_element_type=F32)


def dot_nt(a, b):
    return lax.dot_general(a, b, (((1,), (1,)), ((), ())), preferred_element_type=F32)


def split(x):
    upper = x.astype(BF)
    return upper, (x - upper.astype(F32)).astype(BF)


def rms_norm(values, gain):
    scale = lax.rsqrt(jnp.mean(values * values, axis=-1, keepdims=True) + 1e-06)
    return values * scale * gain


def mixer_body(heads, head_size, *refs):
    count = 16
    sources, (partial_ref, base_ref, aux_ref, extra_ref) = refs[:count], refs[count : count + 4]
    places, sems = refs[count + 4 : 2 * count + 4], refs[2 * count + 4]
    copies = [pltpu.make_async_copy(sources[at], places[at], sems.at[at]) for at in range(count - 1)]
    state_src, state = sources[count - 1], places[count - 1]
    state_copies = [
        pltpu.make_async_copy(state_src.at[:, h], state.at[h], sems.at[count - 1 + h]) for h in range(heads)
    ]
    (tokens, gain, route_ids, route_weights, key_w, query_w, value_w, decay_down, rate_down, decay_up,
     rate_up, decay_base, rate_base, head_gain, out_w) = places[: count - 1]
    for copy in copies[: count - 2] + state_copies + copies[count - 2 :]:
        copy.start()

    for at in range(2, 4):
        copies[at].wait()
    weights = route_weights[...]
    share = weights / jnp.sum(weights, axis=0, keepdims=True) * 2.5
    upper = share.astype(BF).astype(F32)
    info = jnp.concatenate([route_ids[...].astype(F32), upper, share - upper], axis=0)
    lanes = extra_ref.shape[1]
    info = jnp.concatenate([info, jnp.zeros((lanes - info.shape[0], info.shape[1]), F32)], axis=0)
    extra_ref[...] = info.T.astype(BF)

    seqs = tokens.shape[0]
    copies[0].wait()
    copies[1].wait()
    normed = rms_norm(tokens[...].astype(F32), gain[...]).astype(BF)
    copies[4].wait()
    key = dot(normed, key_w[...]).astype(BF).astype(F32)
    copies[5].wait()
    query = dot(normed, query_w[...]).astype(BF).astype(F32)
    copies[6].wait()
    value = dot(normed, value_w[...]).astype(BF).astype(F32)
    for at in range(7, count - 2):
        copies[at].wait()
    decay_low = jnp.tanh(dot_nt(normed, decay_down[...])).astype(BF)
    decay_log = decay_base[...] + dot(decay_low, decay_up[...])
    decay = jnp.exp(-jnp.exp(-0.5) / (1.0 + jnp.exp(-decay_log)))
    rate_low = dot_nt(normed, rate_down[...]).astype(BF)
    rate = 1.0 / (1.0 + jnp.exp(-(rate_base[...] + dot(rate_low, rate_up[...]))))

    def stacked(x):
        return jnp.concatenate([x[:, h * head_size : (h + 1) * head_size] for h in range(heads)], axis=0)

    def shared(x):
        return jnp.sum(x, axis=-1, keepdims=True)

    key, query, value, decay, rate = (stacked(x) for x in (key, query, value, decay, rate))
    read_upper, read_lower = split(decay * query)
    norm = lax.rsqrt(shared(key * key) + 1e-06)
    unit_rate = key * norm * rate
    removed_part = shared(unit_rate * query)
    value_part = shared(key * query)
    for at, x in ((1, unit_rate), (2, decay), (3, key), (4, value)):
        aux_ref[at] = x.reshape(heads, seqs, head_size)
    key = key.astype(BF)

    cols = seqs * head_size
    row = lax.broadcasted_iota(jnp.int32, (seqs, cols), 0)
    lane = lax.broadcasted_iota(jnp.int32, (seqs, cols), 1)
    own = lane // head_size == row

    def fold(x):
        x = jnp.where(own, x, 0.0)
        while x.shape[1] > 2 * head_size:
            half = x.shape[1] // 2
            x = x[:, :half] + x[:, half:]
        return x

    for copy in state_copies:
        copy.wait()
    removed, kept = [], []
    for h in range(heads):
        cut = slice(h * seqs, (h + 1) * seqs)
        rows = jnp.concatenate([key[cut], read_upper[cut], read_lower[cut]], axis=0)
        upper, lower = split(state[h].reshape(cols, head_size))
        both = dot_nt(rows, upper) + dot_nt(rows, lower)
        removed.append(fold(both[:seqs]))
        kept.append(fold(both[seqs : 2 * seqs] + both[2 * seqs :]))
    removed, kept = (jnp.concatenate(x, axis=0) for x in (removed, kept))
    removed = (removed[:, :head_size] + removed[:, head_size:]) * norm
    kept = kept[:, :head_size] + kept[:, head_size:]
    aux_ref[0] = removed.reshape(heads, seqs, head_size)
    read = kept - removed * removed_part + value * value_part
    read = read - jnp.mean(read, axis=-1, keepdims=True)
    read = read * lax.rsqrt(jnp.mean(read * read, axis=-1, keepdims=True) + 0.00064)
    pieces = [read[h * seqs : (h + 1) * seqs] for h in range(heads)]
    mixed = (jnp.concatenate(pieces, axis=1) * head_gain[...]).astype(BF)
    copies[count - 2].wait()
    partial = dot(mixed, out_w[...]).astype(BF)
    partial_ref[...] = partial
    base_ref[...] = tokens[...].astype(F32) + partial.astype(F32)


def mixer(*args):
    seqs, heads, _, head_size = args[-1].shape
    width = args[0].shape[1]
    scratch = [pltpu.VMEM(a.shape, a.dtype) for a in args[:-1]]
    scratch.append(pltpu.VMEM((heads, seqs, head_size, head_size), F32))
    scratch.append(pltpu.SemaphoreType.DMA((len(args) + heads,)))
    return pl.pallas_call(
        lambda *refs: mixer_body(heads, head_size, *refs),
        out_shape=(
            pltpu.VMEM((seqs, width), BF),
            pltpu.VMEM((seqs, width), F32),
            pltpu.VMEM((5, heads, seqs, head_size), F32),
            pltpu.VMEM((seqs, 128), BF),
        ),
        in_specs=[HBM] * len(args),
        out_specs=(VMEM,) * 4,
        scratch_shapes=scratch,
        compiler_params=pltpu.CompilerParams(vmem_limit_bytes=16 * MIB),
        name="mixer",
    )(*(in_hbm(a) for a in args))


def state_body(state_ref, aux_ref, new_ref):
    seqs, _, size, _ = state_ref.shape
    cols = seqs * size
    removed, unit_rate, decay, key, value = (aux_ref[i, pl.program_id(0)] for i in range(5))
    removed_upper, removed_lower = (x.astype(F32) for x in split(removed))
    rate_upper, rate_lower = split(-unit_rate)
    left = jnp.concatenate([removed_upper, removed_lower, removed_upper, value], axis=0)
    right = jnp.concatenate([rate_upper, rate_upper, rate_lower, key.astype(BF)], axis=0)
    row = lax.broadcasted_iota(jnp.int32, (4 * seqs, cols), 0)
    lane = lax.broadcasted_iota(jnp.int32, (4 * seqs, cols), 1)
    left = jnp.where(lane // size == row % seqs, jnp.concatenate([left] * seqs, axis=1), 0.0)
    outer = dot(left.T.astype(BF), right)
    new_ref[:, 0] = state_ref[:, 0] * decay[:, None, :] + outer.reshape(seqs, size, size)


def update_state(state, aux):
    seqs, heads, size, _ = state.shape
    block = pl.BlockSpec((seqs, 1, size, size), lambda h: (0, h, 0, 0))
    return pl.pallas_call(
        state_body,
        grid=(heads,),
        out_shape=jax.ShapeDtypeStruct(state.shape, F32),
        in_specs=[block, VMEM],
        out_specs=block,
        cost_estimate=pl.CostEstimate(
            flops=4 * 64 * state.size, transcendentals=0, bytes_accessed=16 * state.size
        ),
        compiler_params=pltpu.CompilerParams(vmem_limit_bytes=16 * MIB),
        name="state_update",
    )(state, aux)


def pack_body(top, half, base, other, gain, blend_vector, extra, block_ref, resid_ref):
    resid = (base[...] + other[...].astype(F32)).astype(BF).astype(F32)
    mid = rms_norm(resid, gain[...]).astype(BF)
    score = jnp.sum(mid.astype(F32) * blend_vector[...].astype(F32), axis=-1, keepdims=True)
    upper, lower = (x.astype(F32) for x in split(1.0 / (1.0 + jnp.exp(-score))))
    info = extra[...].astype(F32)
    lane = lax.broadcasted_iota(jnp.int32, info.shape, 1)
    info = jnp.where(lane == 3 * top, upper, jnp.where(lane == 3 * top + 1, lower, info))
    first = lax.axis_index("tp") == 0
    block_ref[:, :half] = jnp.where(first, mid[:, :half], mid[:, half:])
    block_ref[:, half:] = info.astype(BF)
    resid_ref[...] = jnp.where(first, resid[:, :half], resid[:, half:])


def pack(base, other, gain, blend_vector, extra, top):
    seqs, width = base.shape
    half = width // 2
    return pl.pallas_call(
        lambda *refs: pack_body(top, half, *refs),
        out_shape=(
            pltpu.VMEM((seqs, half + extra.shape[1]), BF),
            pltpu.VMEM((seqs, half), F32),
        ),
        in_specs=[VMEM] * 5,
        out_specs=(VMEM, VMEM),
        compiler_params=pltpu.CompilerParams(vmem_limit_bytes=4 * MIB),
        name="pack",
    )(base, other, gain, blend_vector, extra)


def ffn_body(pieces, seqs, top, half, *refs):
    places, blocks = refs[:6], refs[6 : 6 + 2 * pieces]
    other_ref, mine_ref = refs[6 + 2 * pieces :]
    near = jnp.concatenate([b[:, :half] for b in blocks[:pieces]], axis=0)
    far = jnp.concatenate([b[:, :half] for b in blocks[pieces:]], axis=0)
    first = lax.axis_index("tp") == 0
    rows = jnp.concatenate([jnp.where(first, near, far), jnp.where(first, far, near)], axis=1)
    info = jnp.concatenate([b[:, half:] for b in blocks[:pieces]], axis=0).astype(F32)
    scalars = info[:, top : 2 * top] + info[:, 2 * top : 3 * top]
    here = lax.axis_index("ep").astype(F32)
    scale = jnp.sum(jnp.where(info[:, :top] == here, scalars, 0.0), axis=1, keepdims=True)
    blend = info[:, 3 * top : 3 * top + 1] + info[:, 3 * top + 1 : 3 * top + 2]

    def hidden(at, by):
        gate = dot_nt(rows, places[at][...])
        up = dot_nt(rows, places[at + 1][...])
        return (gate / (1.0 + jnp.exp(-gate)) * up * by).astype(BF)

    expert = hidden(0, scale)
    dense = hidden(2, blend)
    count = blocks[0].shape[0] // seqs
    chunk = lax.broadcasted_iota(jnp.int32, (near.shape[0], 1), 0) // seqs % count
    side = chunk * 0 + lax.axis_index("tp")
    for bit in range(count.bit_length() - 1):
        side = side ^ (chunk >> bit & 1)
    low = dot(expert, places[4][:, :half]) + dot(dense, places[5][:, :half])
    high = dot(expert, places[4][:, half:]) + dot(dense, places[5][:, half:])
    other_ref[...] = jnp.where(side == 0, high, low).astype(BF)
    mine_ref[...] = jnp.where(side == 0, low, high)


def ffn(weights, near, far, seqs, top):
    rows = sum(b.shape[0] for b in near)
    half = weights[-1].shape[1] // 2
    return pl.pallas_call(
        lambda *refs: ffn_body(len(near), seqs, top, half, *refs),
        out_shape=(pltpu.VMEM((rows, half), BF), pltpu.VMEM((rows, half), F32)),
        in_specs=[VMEM] * (len(weights) + 2 * len(near)),
        out_specs=(VMEM, VMEM),
        compiler_params=pltpu.CompilerParams(vmem_limit_bytes=8 * MIB + rows * 20 * 1024),
        name="ffn",
    )(*weights, *near, *far)


def swap_tp(x):
    count = lax.axis_size("tp")
    return lax.ppermute(x, "tp", [(i, i ^ 1) for i in range(count)])


def cross(x, mask):
    size = lax.axis_size("tp")
    pairs = [
        (i * size + j, (i ^ mask) * size + (j ^ 1)) for i in range(lax.axis_size("ep")) for j in range(size)
    ]
    return lax.ppermute(x, ("ep", "tp"), pairs)


def swap_ep(x, mask):
    count = lax.axis_size("ep")
    return lax.ppermute(x, "ep", [(i, i ^ mask) for i in range(count)])


def shards(
    tokens,
    prior_state,
    first_gain,
    query_weight,
    key_weight,
    value_weight,
    decay_down,
    decay_up,
    decay_base,
    rate_down,
    rate_up,
    rate_base,
    head_gain,
    out_weight,
    mid_gain,
    route_ids,
    route_weights,
    expert_gate,
    expert_up,
    expert_down,
    dense_gate,
    dense_up,
    dense_down,
    blend_vector,
):
    count_ep = lax.axis_size("ep")
    seqs = tokens.shape[0]
    width = tokens.shape[1]
    top_count = route_ids.shape[1]
    half_width = width // 2
    partial_value, base, aux, extra = mixer(
        tokens,
        first_gain,
        route_ids.T,
        route_weights.T,
        key_weight,
        query_weight,
        value_weight,
        decay_down.T,
        rate_down.T,
        decay_up,
        rate_up,
        decay_base,
        rate_base,
        head_gain,
        out_weight,
        prior_state,
    )
    block, resid = pack(base, swap_tp(partial_value), mid_gain, blend_vector, extra, top_count)

    mask = count_ep // 2
    masks = []
    while mask >= 4:
        block = jnp.concatenate([block, swap_ep(block, mask)], axis=0)
        masks.append(mask)
        mask //= 2
    low = [m for m in (1, 3, 2) if m < count_ep]
    near = [block]
    for m in low:
        near.append(swap_ep(block, m))
    far = [swap_tp(b) for b in near]
    rows = sum(b.shape[0] for b in near)

    weights = (
        expert_gate[0].T,
        expert_up[0].T,
        dense_gate.T,
        dense_up.T,
        expert_down[0],
        dense_down,
    )
    other, mine = ffn(weights, near, far, seqs, top_count)
    total = mine + swap_tp(other).astype(F32)

    groups = len(low) + 1
    part = total.reshape((groups, rows // groups, half_width))
    send, aux = lax.optimization_barrier((part.astype(BF), aux))
    new_state = update_state(prior_state, aux)
    back = []
    for i, m in enumerate(low):
        back.append(swap_ep(send[i + 1], m))
    back, new_state = lax.optimization_barrier((back, new_state))
    total = part[0] + sum(x.astype(F32) for x in back)
    for mask in reversed(masks):
        part = total.reshape((2, -1, half_width))
        total = part[0] + cross(part[1].astype(BF), mask).astype(F32)

    mixed = (resid + total).astype(BF)
    return (mixed, new_state)


def solution(mesh):
    in_specs = (
        P("ep", None),
        P("ep", "tp", None, None),
        P(),
        P(None, "tp"),
        P(None, "tp"),
        P(None, "tp"),
        P(),
        P(None, "tp"),
        P("tp"),
        P(),
        P(None, "tp"),
        P("tp"),
        P("tp"),
        P("tp", None),
        P(),
        P("ep", None),
        P("ep", None),
        P("ep", None, "tp"),
        P("ep", None, "tp"),
        P("ep", "tp", None),
        P(None, ("ep", "tp")),
        P(None, ("ep", "tp")),
        P(("ep", "tp"), None),
        P(),
    )
    out_specs = (P("ep", "tp"), P("ep", "tp", None, None))
    step = jax.shard_map(shards, mesh=mesh, in_specs=in_specs, out_specs=out_specs, check_vma=False)
    for turns in (GATHER_TURNS, REDUCE_TURNS):
        turns = [m for m in turns if m < mesh.shape["ep"]]
    return step
```

```python
import jax
import jax.numpy as jnp
from jax import lax
from jax.experimental import pallas as pl
from jax.experimental.pallas import tpu as pltpu
from jax.sharding import PartitionSpec as P

BF = jnp.bfloat16
F32 = jnp.float32
MIB = 1024 * 1024
GATHER_TURNS = (3, 1, 2)
REDUCE_TURNS = (3, 2, 1)


VMEM = pl.BlockSpec(memory_space=pltpu.VMEM)
HBM = pl.BlockSpec(memory_space=pltpu.MemorySpace.HBM)


def in_hbm(x):
    return pltpu.with_memory_space_constraint(x, pltpu.MemorySpace.HBM)


def dot(a, b):
    return jnp.dot(a, b, preferred_element_type=F32)


def dot_nt(a, b):
    return lax.dot_general(a, b, (((1,), (1,)), ((), ())), preferred_element_type=F32)


def split(x):
    upper = x.astype(BF)
    return upper, (x - upper.astype(F32)).astype(BF)


def rms_norm(values, gain):
    scale = lax.rsqrt(jnp.mean(values * values, axis=-1, keepdims=True) + 1e-06)
    return values * scale * gain


def mixer_body(heads, head_size, *refs):
    count = 16
    sources, (partial_ref, base_ref, aux_ref, extra_ref) = refs[:count], refs[count : count + 4]
    places, sems = refs[count + 4 : 2 * count + 4], refs[2 * count + 4]
    copies = [pltpu.make_async_copy(sources[at], places[at], sems.at[at]) for at in range(count - 1)]
    state_src, state = sources[count - 1], places[count - 1]
    state_copies = [
        pltpu.make_async_copy(state_src.at[:, h], state.at[h], sems.at[count - 1 + h]) for h in range(heads)
    ]
    (tokens, gain, route_ids, route_weights, key_w, query_w, value_w, decay_down, rate_down, decay_up,
     rate_up, decay_base, rate_base, head_gain, out_w) = places[: count - 1]
    for copy in copies[: count - 2] + state_copies + copies[count - 2 :]:
        copy.start()

    for at in range(2, 4):
        copies[at].wait()
    weights = route_weights[...]
    share = weights / jnp.sum(weights, axis=0, keepdims=True) * 2.5
    upper = share.astype(BF).astype(F32)
    info = jnp.concatenate([route_ids[...].astype(F32), upper, share - upper], axis=0)
    lanes = extra_ref.shape[1]
    info = jnp.concatenate([info, jnp.zeros((lanes - info.shape[0], info.shape[1]), F32)], axis=0)
    extra_ref[...] = info.T.astype(BF)

    seqs = tokens.shape[0]
    copies[0].wait()
    copies[1].wait()
    normed = rms_norm(tokens[...].astype(F32), gain[...]).astype(BF)
    copies[4].wait()
    key = dot(normed, key_w[...]).astype(BF).astype(F32)
    copies[5].wait()
    query = dot(normed, query_w[...]).astype(BF).astype(F32)
    copies[6].wait()
    value = dot(normed, value_w[...]).astype(BF).astype(F32)
    for at in range(7, count - 2):
        copies[at].wait()
    decay_low = jnp.tanh(dot_nt(normed, decay_down[...])).astype(BF)
    decay_log = decay_base[...] + dot(decay_low, decay_up[...])
    decay = jnp.exp(-jnp.exp(-0.5) / (1.0 + jnp.exp(-decay_log)))
    rate_low = dot_nt(normed, rate_down[...]).astype(BF)
    rate = 1.0 / (1.0 + jnp.exp(-(rate_base[...] + dot(rate_low, rate_up[...]))))

    def stacked(x):
        return jnp.concatenate([x[:, h * head_size : (h + 1) * head_size] for h in range(heads)], axis=0)

    def shared(x):
        return jnp.sum(x, axis=-1, keepdims=True)

    key, query, value, decay, rate = (stacked(x) for x in (key, query, value, decay, rate))
    read_upper, read_lower = split(decay * query)
    norm = lax.rsqrt(shared(key * key) + 1e-06)
    unit_rate = key * norm * rate
    removed_part = shared(unit_rate * query)
    value_part = shared(key * query)
    for at, x in ((1, unit_rate), (2, decay), (3, key), (4, value)):
        aux_ref[at] = x.reshape(heads, seqs, head_size)
    key = key.astype(BF)

    cols = seqs * head_size
    row = lax.broadcasted_iota(jnp.int32, (seqs, cols), 0)
    lane = lax.broadcasted_iota(jnp.int32, (seqs, cols), 1)
    own = lane // head_size == row

    def fold(x):
        x = jnp.where(own, x, 0.0)
        while x.shape[1] > 2 * head_size:
            half = x.shape[1] // 2
            x = x[:, :half] + x[:, half:]
        return x

    for copy in state_copies:
        copy.wait()
    removed, kept = [], []
    for h in range(heads):
        cut = slice(h * seqs, (h + 1) * seqs)
        rows = jnp.concatenate([key[cut], read_upper[cut], read_lower[cut]], axis=0)
        upper, lower = split(state[h].reshape(cols, head_size))
        both = dot_nt(rows, upper) + dot_nt(rows, lower)
        removed.append(fold(both[:seqs]))
        kept.append(fold(both[seqs : 2 * seqs] + both[2 * seqs :]))
    removed, kept = (jnp.concatenate(x, axis=0) for x in (removed, kept))
    removed = (removed[:, :head_size] + removed[:, head_size:]) * norm
    kept = kept[:, :head_size] + kept[:, head_size:]
    aux_ref[0] = removed.reshape(heads, seqs, head_size)
    read = kept - removed * removed_part + value * value_part
    read = read - jnp.mean(read, axis=-1, keepdims=True)
    read = read * lax.rsqrt(jnp.mean(read * read, axis=-1, keepdims=True) + 0.00064)
    pieces = [read[h * seqs : (h + 1) * seqs] for h in range(heads)]
    mixed = (jnp.concatenate(pieces, axis=1) * head_gain[...]).astype(BF)
    copies[count - 2].wait()
    partial = dot(mixed, out_w[...]).astype(BF)
    partial_ref[...] = partial
    base_ref[...] = tokens[...].astype(F32) + partial.astype(F32)


def mixer(*args):
    seqs, heads, _, head_size = args[-1].shape
    width = args[0].shape[1]
    scratch = [pltpu.VMEM(a.shape, a.dtype) for a in args[:-1]]
    scratch.append(pltpu.VMEM((heads, seqs, head_size, head_size), F32))
    scratch.append(pltpu.SemaphoreType.DMA((len(args) + heads,)))
    return pl.pallas_call(
        lambda *refs: mixer_body(heads, head_size, *refs),
        out_shape=(
            pltpu.VMEM((seqs, width), BF),
            pltpu.VMEM((seqs, width), F32),
            pltpu.VMEM((5, heads, seqs, head_size), F32),
            pltpu.VMEM((seqs, 128), BF),
        ),
        in_specs=[HBM] * len(args),
        out_specs=(VMEM,) * 4,
        scratch_shapes=scratch,
        compiler_params=pltpu.CompilerParams(vmem_limit_bytes=16 * MIB),
        name="mixer",
    )(*(in_hbm(a) for a in args))


def state_body(state_ref, aux_ref, new_ref):
    seqs, _, size, _ = state_ref.shape
    cols = seqs * size
    removed, unit_rate, decay, key, value = (aux_ref[i, pl.program_id(0)] for i in range(5))
    removed_upper, removed_lower = (x.astype(F32) for x in split(removed))
    rate_upper, rate_lower = split(-unit_rate)
    left = jnp.concatenate([removed_upper, removed_lower, removed_upper, value], axis=0)
    right = jnp.concatenate([rate_upper, rate_upper, rate_lower, key.astype(BF)], axis=0)
    row = lax.broadcasted_iota(jnp.int32, (4 * seqs, cols), 0)
    lane = lax.broadcasted_iota(jnp.int32, (4 * seqs, cols), 1)
    left = jnp.where(lane // size == row % seqs, jnp.concatenate([left] * seqs, axis=1), 0.0)
    outer = dot(left.T.astype(BF), right)
    new_ref[:, 0] = state_ref[:, 0] * decay[:, None, :] + outer.reshape(seqs, size, size)


def update_state(state, aux):
    seqs, heads, size, _ = state.shape
    block = pl.BlockSpec((seqs, 1, size, size), lambda h: (0, h, 0, 0))
    return pl.pallas_call(
        state_body,
        grid=(heads,),
        out_shape=jax.ShapeDtypeStruct(state.shape, F32),
        in_specs=[block, VMEM],
        out_specs=block,
        cost_estimate=pl.CostEstimate(
            flops=4 * 64 * state.size, transcendentals=0, bytes_accessed=16 * state.size
        ),
        compiler_params=pltpu.CompilerParams(vmem_limit_bytes=16 * MIB),
        name="state_update",
    )(state, aux)


def pack_body(top, half, base, other, gain, blend_vector, extra, block_ref, resid_ref):
    resid = (base[...] + other[...].astype(F32)).astype(BF).astype(F32)
    mid = rms_norm(resid, gain[...]).astype(BF)
    score = jnp.sum(mid.astype(F32) * blend_vector[...].astype(F32), axis=-1, keepdims=True)
    upper, lower = (x.astype(F32) for x in split(1.0 / (1.0 + jnp.exp(-score))))
    info = extra[...].astype(F32)
    lane = lax.broadcasted_iota(jnp.int32, info.shape, 1)
    info = jnp.where(lane == 3 * top, upper, jnp.where(lane == 3 * top + 1, lower, info))
    first = lax.axis_index("tp") == 0
    block_ref[:, :half] = jnp.where(first, mid[:, :half], mid[:, half:])
    block_ref[:, half:] = info.astype(BF)
    resid_ref[...] = jnp.where(first, resid[:, :half], resid[:, half:])


def pack(base, other, gain, blend_vector, extra, top):
    seqs, width = base.shape
    half = width // 2
    return pl.pallas_call(
        lambda *refs: pack_body(top, half, *refs),
        out_shape=(
            pltpu.VMEM((seqs, half + extra.shape[1]), BF),
            pltpu.VMEM((seqs, half), F32),
        ),
        in_specs=[VMEM] * 5,
        out_specs=(VMEM, VMEM),
        compiler_params=pltpu.CompilerParams(vmem_limit_bytes=4 * MIB),
        name="pack",
    )(base, other, gain, blend_vector, extra)


def prefetch_body(*refs):
    sources, places, sems = refs[:6], refs[6:9], refs[9]
    copies = []
    for at in range(6):
        count = sources[at].shape[0]
        copies.append(
            pltpu.make_async_copy(sources[at], places[at // 2].at[pl.ds(at % 2 * count, count)], sems.at[at])
        )
    for copy in copies:
        copy.start()
    for copy in copies:
        copy.wait()


def prefetch(weights):
    return pl.pallas_call(
        prefetch_body,
        out_shape=tuple(pltpu.VMEM((2 * w.shape[0], w.shape[1]), w.dtype) for w in weights[::2]),
        in_specs=[HBM] * 6,
        out_specs=(VMEM,) * 3,
        scratch_shapes=[pltpu.SemaphoreType.DMA((6,))],
        compiler_params=pltpu.CompilerParams(vmem_limit_bytes=4 * MIB),
        name="prefetch",
    )(*(in_hbm(w) for w in weights))


def ffn_body(pieces, seqs, top, half, *refs):
    places, blocks = refs[:3], refs[3 : 3 + 2 * pieces]
    other_ref, mine_ref = refs[3 + 2 * pieces :]
    near = jnp.concatenate([b[:, :half] for b in blocks[:pieces]], axis=0)
    far = jnp.concatenate([b[:, :half] for b in blocks[pieces:]], axis=0)
    first = lax.axis_index("tp") == 0
    rows = jnp.concatenate([jnp.where(first, near, far), jnp.where(first, far, near)], axis=1)
    info = jnp.concatenate([b[:, half:] for b in blocks[:pieces]], axis=0).astype(F32)
    scalars = info[:, top : 2 * top] + info[:, 2 * top : 3 * top]
    here = lax.axis_index("ep").astype(F32)
    scale = jnp.sum(jnp.where(info[:, :top] == here, scalars, 0.0), axis=1, keepdims=True)
    blend = info[:, 3 * top : 3 * top + 1] + info[:, 3 * top + 1 : 3 * top + 2]

    gate = dot_nt(rows, places[0][...])
    up = dot_nt(rows, places[1][...])
    unit = lax.broadcasted_iota(jnp.int32, gate.shape, 1)
    by = jnp.where(unit < gate.shape[1] // 2, scale, blend)
    hidden = (gate / (1.0 + jnp.exp(-gate)) * up * by).astype(BF)
    count = blocks[0].shape[0] // seqs
    chunk = lax.broadcasted_iota(jnp.int32, (near.shape[0], 1), 0) // seqs % count
    side = chunk * 0 + lax.axis_index("tp")
    for bit in range(count.bit_length() - 1):
        side = side ^ (chunk >> bit & 1)
    low = dot(hidden, places[2][:, :half])
    high = dot(hidden, places[2][:, half:])
    other_ref[...] = jnp.where(side == 0, high, low).astype(BF)
    mine_ref[...] = jnp.where(side == 0, low, high)


def ffn(weights, near, far, seqs, top):
    rows = sum(b.shape[0] for b in near)
    half = weights[-1].shape[1] // 2
    return pl.pallas_call(
        lambda *refs: ffn_body(len(near), seqs, top, half, *refs),
        out_shape=(pltpu.VMEM((rows, half), BF), pltpu.VMEM((rows, half), F32)),
        in_specs=[VMEM] * (len(weights) + 2 * len(near)),
        out_specs=(VMEM, VMEM),
        compiler_params=pltpu.CompilerParams(vmem_limit_bytes=8 * MIB + rows * 20 * 1024),
        name="ffn",
    )(*weights, *near, *far)


def swap_tp(x):
    count = lax.axis_size("tp")
    return lax.ppermute(x, "tp", [(i, i ^ 1) for i in range(count)])


def cross(x, mask):
    size = lax.axis_size("tp")
    pairs = [
        (i * size + j, (i ^ mask) * size + (j ^ 1)) for i in range(lax.axis_size("ep")) for j in range(size)
    ]
    return lax.ppermute(x, ("ep", "tp"), pairs)


def swap_ep(x, mask):
    count = lax.axis_size("ep")
    return lax.ppermute(x, "ep", [(i, i ^ mask) for i in range(count)])


def shards(
    tokens,
    prior_state,
    first_gain,
    query_weight,
    key_weight,
    value_weight,
    decay_down,
    decay_up,
    decay_base,
    rate_down,
    rate_up,
    rate_base,
    head_gain,
    out_weight,
    mid_gain,
    route_ids,
    route_weights,
    expert_gate,
    expert_up,
    expert_down,
    dense_gate,
    dense_up,
    dense_down,
    blend_vector,
):
    count_ep = lax.axis_size("ep")
    seqs = tokens.shape[0]
    width = tokens.shape[1]
    top_count = route_ids.shape[1]
    half_width = width // 2
    partial_value, base, aux, extra = mixer(
        tokens,
        first_gain,
        route_ids.T,
        route_weights.T,
        key_weight,
        query_weight,
        value_weight,
        decay_down.T,
        rate_down.T,
        decay_up,
        rate_up,
        decay_base,
        rate_base,
        head_gain,
        out_weight,
        prior_state,
    )
    block, resid = pack(base, swap_tp(partial_value), mid_gain, blend_vector, extra, top_count)

    weights = (
        expert_gate[0].T,
        dense_gate.T,
        expert_up[0].T,
        dense_up.T,
        expert_down[0],
        dense_down,
    )
    block, *weights = lax.optimization_barrier((block, *weights))
    weights = prefetch(weights)
    mask = count_ep // 2
    masks = []
    while mask >= 4:
        arrived = swap_ep(block, mask)
        if not masks:
            arrived, *weights = lax.optimization_barrier((arrived, *weights))
        block = jnp.concatenate([block, arrived], axis=0)
        masks.append(mask)
        mask //= 2
    low = [m for m in (1, 3, 2) if m < count_ep]
    near = [block]
    for m in low:
        near.append(swap_ep(block, m))
    far = [swap_tp(b) for b in near]
    rows = sum(b.shape[0] for b in near)

    other, mine = ffn(weights, near, far, seqs, top_count)
    total = mine + swap_tp(other).astype(F32)

    groups = len(low) + 1
    part = total.reshape((groups, rows // groups, half_width))
    send, aux = lax.optimization_barrier((part.astype(BF), aux))
    new_state = update_state(prior_state, aux)
    back = []
    for i, m in enumerate(low):
        back.append(swap_ep(send[i + 1], m))
    back, new_state = lax.optimization_barrier((back, new_state))
    total = part[0] + sum(x.astype(F32) for x in back)
    for mask in reversed(masks):
        part = total.reshape((2, -1, half_width))
        total = part[0] + cross(part[1].astype(BF), mask).astype(F32)

    mixed = (resid + total).astype(BF)
    return (mixed, new_state)


def solution(mesh):
    in_specs = (
        P("ep", None),
        P("ep", "tp", None, None),
        P(),
        P(None, "tp"),
        P(None, "tp"),
        P(None, "tp"),
        P(),
        P(None, "tp"),
        P("tp"),
        P(),
        P(None, "tp"),
        P("tp"),
        P("tp"),
        P("tp", None),
        P(),
        P("ep", None),
        P("ep", None),
        P("ep", None, "tp"),
        P("ep", None, "tp"),
        P("ep", "tp", None),
        P(None, ("ep", "tp")),
        P(None, ("ep", "tp")),
        P(("ep", "tp"), None),
        P(),
    )
    out_specs = (P("ep", "tp"), P("ep", "tp", None, None))
    step = jax.shard_map(shards, mesh=mesh, in_specs=in_specs, out_specs=out_specs, check_vma=False)
    for turns in (GATHER_TURNS, REDUCE_TURNS):
        turns = [m for m in turns if m < mesh.shape["ep"]]
    return step
```
